256 devices in a mesh: ep: 64 (over z, y, core), tp: 4 (over x).
Axes of the slice: x: 4, y: 4, z: 8, core: 2. Of those that a mesh axis runs over, the one named last changes fastest.
Arguments:
- tokens: bfloat16 [1536, 1024], P('ep'), may hold values from -1.796875 to 1.796875
- attn_gain: float32 [1024], replicated, may hold values from 0.1 to 1.9
- w_query: bfloat16 [1024, 1024], P(None, 'tp'), may hold values from -0.1875 to 0.1875
- w_key: bfloat16 [1024, 256], P(None, 'tp'), may hold values from -0.1875 to 0.1875
- w_value: bfloat16 [1024, 256], P(None, 'tp'), may hold values from -0.1875 to 0.1875
- w_forget: bfloat16 [1024, 4], P(None, 'tp'), may hold values from -0.1875 to 0.1875
- forget_bias: float32 [4], P('tp'), may hold values from -1 to 2
- query_gain: float32 [64], replicated, may hold values from 0.1 to 1.9
- key_gain: float32 [64], replicated, may hold values from 0.1 to 1.9
- cache_pairs: bfloat16 [1536, 4, 1024, 128], P('ep', 'tp'), may hold values from -6 to 206
- cache_cum: float32 [1536, 4, 1024], P('ep', 'tp'), may hold values from -1024 to 0, as said below
- lengths: int32 [1536], P('ep'), may hold values from 64 to 1024, as said below
- w_output: bfloat16 [1024, 1024], P('tp'), may hold values from -0.1875 to 0.1875
- ffn_gain: float32 [1024], replicated, may hold values from 0.1 to 1.9
- expert_ids: int32 [1536, 2], replicated, may hold values from 0 to 63, all different within a row; in each aligned block of 24 rows (0 to 23, 24 to 47, ...) at most 2 rows name the same one
- route_weight: float32 [1536, 2], replicated, may hold values from 0.2 to 1
- w_exp_gate: bfloat16 [64, 1024, 3584], P('ep', None, 'tp'), may hold values from -0.1875 to 0.1875
- w_exp_up: bfloat16 [64, 1024, 3584], P('ep', None, 'tp'), may hold values from -0.1875 to 0.1875
- w_exp_down: bfloat16 [64, 3584, 1024], P('ep', 'tp'), may hold values from -0.09375 to 0.09375
- shared_gate: bfloat16 [1024], replicated, may hold values from -0.1875 to 0.1875
- w_dense_gate: bfloat16 [4096, 1024], P('ep'), may hold values from -0.1875 to 0.1875
- w_dense_up: bfloat16 [4096, 1024], P('ep'), may hold values from -0.1875 to 0.1875
- w_dense_down: bfloat16 [4096, 1024], P('ep', 'tp'), may hold values from -0.09375 to 0.09375
Outputs:
- layer_out: bfloat16 [1536, 1024], P('ep', 'tp')
The draws below stay inside these ranges and needn't reach their ends.
Inputs may be any that keep to these rules, and one draw needn't show every extreme that they name: The cache of sequence b holds positions 0 to lengths[b] - 1; some sequence has 1024. `expert_ids`: each row names 2 different experts; in each aligned block of 24 rows no expert is named by more than 2 rows. cache_cum[b, g, s] never rises with s.
All inputs are finite; a program needn't handle non-finite values.
Results may differ from the reference program's by a relative error of at most 0.02.
Values may be sent and summed in bfloat16 or wider, within the bound.
No kernel may reach another device: no remote copies, remote signals or barrier semaphores. Data moves between devices by JAX's collectives and lax.ppermute only.
A program may use at most 64 MiB of HBM per device.

```python
import math
import jax
import jax.numpy as jnp
import numpy as np
from jax import lax

D = 1024
HEADS = 16
HEAD_DIM = 64
KV_HEADS = 4
FF_EXPERT = 3584
DENSE_FF = 4096
TOP_K = 2
SEQ_GRP = 24
CACHE_SLOTS = 1024
BATCH = 1536
EXPERTS = 64
CAP = 2
HEAD_GROUP = 4
N_EP = 64
N_TP = 4


def draw_lengths(key, part):
    lengths_drawn = jax.random.randint(key, (BATCH,), CACHE_SLOTS // 16, CACHE_SLOTS + 1, dtype=jnp.int32)
    return lengths_drawn.at[0].set(CACHE_SLOTS)


def draw_cache_pairs(key, part):
    base_key = jax.random.fold_in(key, 0)
    complete_shape = (BATCH, KV_HEADS, CACHE_SLOTS, 2 * HEAD_DIM)
    entries = jnp.clip(jax.random.normal(base_key, complete_shape, jnp.float32), -6.0, 6.0)
    return entries.astype(jnp.bfloat16)


def draw_cache_cum(key, part):
    key_sequence = jax.random.split(key, 8)
    complete_shape = (BATCH, KV_HEADS, CACHE_SLOTS)
    head_shape = (BATCH, KV_HEADS, 1)
    slow_share = 0.5
    sluggish_flag = jax.random.uniform(key_sequence[0], head_shape) < slow_share
    whole_rate = jnp.exp(jax.random.uniform(key_sequence[1], head_shape, jnp.float32, jnp.log(0.4), jnp.log(2.0))) / CACHE_SLOTS
    quick_rate = 1.0 / jax.random.uniform(key_sequence[2], head_shape, jnp.float32, 30.0, 50.0)
    step_frequency = jnp.where(sluggish_flag, whole_rate, quick_rate)
    device_multiplier = jnp.exp(jax.random.uniform(key_sequence[3], head_shape, jnp.float32, jnp.log(0.5), jnp.log(2.0)))
    block_multiplier = jnp.exp(jax.random.uniform(key_sequence[4], (BATCH, KV_HEADS, 8), jnp.float32, jnp.log(0.5), jnp.log(2.0)))
    block_multiplier = jnp.repeat(block_multiplier, CACHE_SLOTS // 8, axis=2)
    coarse_multiplier = jax.random.uniform(key_sequence[5], complete_shape, jnp.float32, 0.5, 2.0)
    spike_flag = (jax.random.uniform(key_sequence[6], complete_shape) < 3.0 / CACHE_SLOTS) & sluggish_flag
    spike_penalty = jnp.log(jax.random.uniform(key_sequence[7], complete_shape, jnp.float32, 0.5, 0.8))
    gate_logarithms = -step_frequency * device_multiplier * block_multiplier * coarse_multiplier + jnp.where(spike_flag, spike_penalty, 0.0)
    return jnp.cumsum(gate_logarithms, axis=2)


def block_levels(key, shape, shards, smallest, high):
    loudness, own = 1.0, jax.random.fold_in(key, 6)
    for axis_at, parts in shards:
        heights = jnp.exp(jax.random.uniform(jax.random.fold_in(own, axis_at), (parts,), jnp.float32, smallest / len(shards), high / len(shards)))
        loudness = loudness * jnp.repeat(heights, shape[axis_at] // parts).reshape([-1 if axis == axis_at else 1 for axis in range(len(shape))])
    return loudness


def routed_block(stream_key, own, number, rows, amount, top, reach, slope):
    sequence = jax.random.permutation(stream_key, amount)
    crowded, common = shares(amount, rows * top, reach, slope, True), shares(amount, rows * top, reach, slope, False)
    places = jnp.arange(amount)

    def named(sizes, rotation):
        used = int((sizes > 0).sum())
        fixed = max(1, used // 4)
        shifted = fixed + (places - fixed + rotation * (used - fixed)) % max(1, amount - fixed)
        return jnp.zeros((amount,), jnp.int32).at[sequence[jnp.where(places < fixed, places, shifted)]].set(jnp.asarray(sizes, jnp.int32))

    sizes = jnp.where(number % 4 == 0, named(crowded, number // 4), named(common, number - number // 4 - 1))
    mixed = jax.random.permutation(jax.random.fold_in(own, 3), amount)
    giver, taker = mixed[0:amount // 2 * 2:2], mixed[1:amount // 2 * 2:2]
    slack = jnp.minimum(sizes[giver] - 1, reach - sizes[taker]) // 2
    slack = jnp.where((giver == sequence[0]) | (taker == sequence[0]) | (sizes[taker] == 0), 0, jnp.maximum(slack, 0))
    shifted = jax.random.randint(jax.random.fold_in(own, 4), (amount // 2,), 0, 1 << 20) % (slack + 1)
    sizes = sizes.at[giver].add(-shifted).at[taker].add(shifted)
    members = jnp.searchsorted(jnp.cumsum(sizes), jnp.arange(rows * top), side="right").astype(jnp.int32)
    listing = members.reshape(top, rows).T
    listing = listing[jax.random.permutation(jax.random.fold_in(own, 1), rows)]
    rotation = jax.random.randint(jax.random.fold_in(own, 2), (rows, 1), 0, top)
    return jnp.take_along_axis(listing, (jnp.arange(top)[None, :] + rotation) % top, axis=1)


def shares(number_of, total, reach, lean, full):
    weights = [(1 << 20) // math.isqrt(rank ** lean) + 1 for rank in range(1, number_of + 1)]
    largest = reach if full else min(reach, max(-(-total // number_of), total * weights[0] // sum(weights)))
    least = 1 if total - largest >= number_of - 1 else 0
    given, spare = [largest] + [least] * (number_of - 1), total - largest - least * (number_of - 1)
    while spare > 0:
        candidates = [i for i in range(1, number_of) if given[i] < largest] or [i for i in range(1, number_of) if given[i] < reach]
        whole, budget = sum([weights[i] for i in candidates]), spare
        for i in candidates:
            extra = min(reach - given[i], max(1, budget * weights[i] // whole), spare)
            given[i] = given[i] + extra
            spare = spare - extra
    return np.array(given)


def bell_draw(rng, extent, scale, most, shards=(), held_as=jnp.bfloat16):
    gain = block_levels(rng, extent, shards, -0.22, 0.18) if shards else 1.0
    result = jax.random.normal(rng, extent, jnp.float32) * scale * gain
    return jnp.minimum(jnp.maximum(result, -most), most).astype(held_as)


def setup_inputs(seed: int = 0) -> dict:
    keys = jax.random.split(jax.random.key(seed), 24)
    tokens = bell_draw(keys[0], (BATCH, D), 0.3, 1.796875, ((0, 64),))
    attn_gain = jnp.clip(1.0 + 0.18 * jax.random.normal(keys[1], (D,), jnp.float32), 0.1, 1.9)
    w_query = bell_draw(keys[2], (D, HEADS * HEAD_DIM), D ** -0.5, 0.1875, ((1, 4),))
    w_key = bell_draw(keys[3], (D, KV_HEADS * HEAD_DIM), D ** -0.5, 0.1875, ((1, 4),))
    w_value = bell_draw(keys[4], (D, KV_HEADS * HEAD_DIM), D ** -0.5, 0.1875, ((1, 4),))
    w_forget = bell_draw(keys[5], (D, KV_HEADS), D ** -0.5, 0.1875, ((1, 4),))
    forget_bias = jnp.clip(-1.0 + 3.0 * jax.random.uniform(keys[6], (KV_HEADS,), jnp.float32) ** block_levels(keys[6], (KV_HEADS,), ((0, 4),), -0.2, 0.2), -1.0, 2.0)
    query_gain = jnp.clip(1.0 + 0.18 * jax.random.normal(keys[7], (HEAD_DIM,), jnp.float32), 0.1, 1.9)
    key_gain = jnp.clip(1.0 + 0.18 * jax.random.normal(keys[8], (HEAD_DIM,), jnp.float32), 0.1, 1.9)
    cache_pairs = draw_cache_pairs(jax.random.fold_in(keys[23], 71), 0)
    cache_cum = draw_cache_cum(jax.random.fold_in(keys[23], 71), 0)
    lengths = draw_lengths(jax.random.fold_in(keys[23], 71), 0)
    w_output = bell_draw(keys[12], (HEADS * HEAD_DIM, D), (HEADS * HEAD_DIM) ** -0.5, 0.1875, ((0, 4),))
    ffn_gain = jnp.clip(1.0 + 0.18 * jax.random.normal(keys[13], (D,), jnp.float32), 0.1, 1.9)
    expert_ids_keys = jax.random.split(jax.random.fold_in(keys[14], 1), BATCH // SEQ_GRP)
    expert_ids_turns = jax.random.permutation(jax.random.fold_in(keys[14], 3), BATCH // SEQ_GRP)
    expert_ids = jax.vmap(lambda own, number: routed_block(jax.random.fold_in(keys[14], 2), own, number, SEQ_GRP, EXPERTS, TOP_K, CAP, 2))(expert_ids_keys, expert_ids_turns).reshape((BATCH, TOP_K))
    route_weight = jnp.clip(jax.random.uniform(keys[15], (BATCH, TOP_K), jnp.float32, 0.2, 1.0), 0.2, 1.0)
    w_exp_gate = bell_draw(keys[16], (EXPERTS, D, FF_EXPERT), D ** -0.5, 0.1875, ((0, 64), (2, 4)))
    w_exp_up = bell_draw(keys[17], (EXPERTS, D, FF_EXPERT), D ** -0.5, 0.1875, ((0, 64), (2, 4)))
    w_exp_down = bell_draw(keys[18], (EXPERTS, FF_EXPERT, D), FF_EXPERT ** -0.5, 0.09375, ((0, 64), (1, 4)))
    shared_gate = bell_draw(keys[19], (D,), D ** -0.5, 0.1875)
    w_dense_gate = bell_draw(keys[20], (DENSE_FF, D), D ** -0.5, 0.1875, ((0, 64),))
    w_dense_up = bell_draw(keys[21], (DENSE_FF, D), D ** -0.5, 0.1875, ((0, 64),))
    w_dense_down = bell_draw(keys[22], (DENSE_FF, D), DENSE_FF ** -0.5, 0.09375, ((0, 64), (1, 4)))
    return dict(tokens=tokens, attn_gain=attn_gain, w_query=w_query, w_key=w_key, w_value=w_value, w_forget=w_forget, forget_bias=forget_bias, query_gain=query_gain, key_gain=key_gain, cache_pairs=cache_pairs, cache_cum=cache_cum, lengths=lengths, w_output=w_output, ffn_gain=ffn_gain, expert_ids=expert_ids, route_weight=route_weight, w_exp_gate=w_exp_gate, w_exp_up=w_exp_up, w_exp_down=w_exp_down, shared_gate=shared_gate, w_dense_gate=w_dense_gate, w_dense_up=w_dense_up, w_dense_down=w_dense_down)


EPSILON = 1e-06

def rms_scale(values, gain_row):
    mean_square = lax.optimization_barrier(jnp.mean(values * values, axis=-1, keepdims=True))
    return values * lax.rsqrt(mean_square + EPSILON) * gain_row

def stored(values):
    return lax.optimization_barrier(values.astype(jnp.bfloat16))

def rounded(values):
    return stored(values).astype(jnp.float32)

def attend(per_block):
    query_rows, fresh_key, value_new, now_cum, cache_block, cum_block, length = per_block
    head_size = query_rows.shape[-1]
    position = jnp.arange(cache_block.shape[2], dtype=jnp.int32)
    is_live = position[None, None, :] < length[:, None, None]
    cached_keys = cache_block[..., :head_size].astype(jnp.float32)
    cached_values = cache_block[..., head_size:].astype(jnp.float32)
    score_multiplier = head_size ** (-0.5)
    past_score = jnp.einsum('bkgd,bkld->bkgl', query_rows, cached_keys) * score_multiplier
    past_score = past_score + (now_cum[:, :, None] - cum_block)[:, :, None, :]
    past_score = jnp.where(is_live[:, :, None, :], past_score, -jnp.inf)
    current_score = jnp.einsum('nlte,nle->nlt', query_rows, fresh_key) * score_multiplier
    row_peak = jnp.maximum(lax.optimization_barrier(jnp.max(past_score, axis=3)), current_score)
    past_exp = jnp.exp(past_score - row_peak[..., None])
    own_exp = jnp.exp(current_score - row_peak)
    denom_sum = lax.optimization_barrier(jnp.sum(past_exp, axis=3)) + own_exp
    past_prob = rounded(past_exp / denom_sum[..., None])
    own_prob = rounded(own_exp / denom_sum)
    head_mix = jnp.einsum('bkgl,bkld->bkgd', past_prob, cached_values)
    head_mix = head_mix + own_prob[..., None] * value_new[:, :, None, :]
    return stored(head_mix)

def reference(tokens, attn_gain, w_query, w_key, w_value, w_forget, forget_bias, query_gain, key_gain, cache_pairs, cache_cum, lengths, w_output, ffn_gain, expert_ids, route_weight, w_exp_gate, w_exp_up, w_exp_down, shared_gate, w_dense_gate, w_dense_up, w_dense_down):
    tokens_f = tokens.astype(jnp.float32)
    normed = stored(rms_scale(tokens_f, attn_gain))
    group_size = HEADS // KV_HEADS
    query_raw = jnp.dot(normed, w_query, preferred_element_type=jnp.float32)
    query_rows = rounded(rms_scale(query_raw.reshape(BATCH, KV_HEADS, group_size, HEAD_DIM), query_gain))
    key_raw = jnp.dot(normed, w_key, preferred_element_type=jnp.float32).reshape(BATCH, KV_HEADS, HEAD_DIM)
    fresh_key = rounded(rms_scale(key_raw, key_gain))
    value_new = rounded(jnp.dot(normed, w_value, preferred_element_type=jnp.float32))
    value_new = value_new.reshape(BATCH, KV_HEADS, HEAD_DIM)
    log_gate = jax.nn.log_sigmoid(jnp.dot(normed, w_forget, preferred_element_type=jnp.float32) + forget_bias)
    last_index = jnp.broadcast_to((lengths - 1)[:, None, None], (BATCH, KV_HEADS, 1)).astype(jnp.int32)
    last_cum = jnp.take_along_axis(cache_cum, last_index, axis=2)[:, :, 0]
    now_cum = last_cum + log_gate

    def to_blocks(values):
        return values.reshape((N_EP, SEQ_GRP) + values.shape[1:])
    head_mix = lax.map(attend, tuple((to_blocks(item) for item in (query_rows, fresh_key, value_new, now_cum, cache_pairs, cache_cum, lengths))))
    head_mix = head_mix.reshape(BATCH, HEADS * HEAD_DIM)
    head_span = HEAD_GROUP * HEAD_DIM
    attn_out = jnp.zeros((BATCH, D), jnp.float32)
    for member in range(N_TP):
        partial_value = jnp.dot(head_mix[:, member * head_span:(member + 1) * head_span], w_output[member * head_span:(member + 1) * head_span], preferred_element_type=jnp.float32)
        attn_out = attn_out + rounded(partial_value)
    residual = stored(tokens_f + attn_out)
    residual_f = residual.astype(jnp.float32)
    normed_two = stored(rms_scale(residual_f, ffn_gain))
    grouped_f = normed_two.astype(jnp.float32).reshape(N_EP, SEQ_GRP, D)
    gate_raw = jnp.dot(normed_two, w_dense_gate.T, preferred_element_type=jnp.float32)
    up_raw = jnp.dot(normed_two, w_dense_up.T, preferred_element_type=jnp.float32)
    dense_hidden = stored(jax.nn.silu(gate_raw) * up_raw)
    mix_gate = jax.nn.sigmoid(jnp.dot(normed_two, shared_gate, preferred_element_type=jnp.float32))
    dense_out = mix_gate[:, None] * jnp.dot(dense_hidden, w_dense_down, preferred_element_type=jnp.float32)
    unit_span = FF_EXPERT // N_TP

    def expert_step(running, expert_item):
        member_id, gate_w, up_w, down_w = expert_item
        chosen = expert_ids == member_id
        is_hit = lax.optimization_barrier(jnp.sum(chosen.astype(jnp.int32), axis=1)).reshape(N_EP, SEQ_GRP)
        weight = lax.optimization_barrier(jnp.sum(jnp.where(chosen, route_weight, 0.0), axis=1))
        slot_rank = jnp.cumsum(is_hit, axis=1)
        slot_ids = jnp.arange(1, CAP + 1, dtype=jnp.int32)[None, :, None]
        picker = ((slot_rank[:, None, :] == slot_ids) & (is_hit[:, None, :] == 1)).astype(jnp.float32)
        picked = jnp.einsum('scn,snd->scd', picker, grouped_f).reshape(N_EP * CAP, D).astype(jnp.bfloat16)
        gate_part = jnp.dot(picked, gate_w, preferred_element_type=jnp.float32)
        up_part = jnp.dot(picked, up_w, preferred_element_type=jnp.float32)
        hidden = stored(jax.nn.silu(gate_part) * up_part)
        expert_rows = jnp.zeros((N_EP * CAP, D), jnp.float32)
        for member in range(N_TP):
            partial_value = jnp.dot(hidden[:, member * unit_span:(member + 1) * unit_span], down_w[member * unit_span:(member + 1) * unit_span], preferred_element_type=jnp.float32)
            expert_rows = expert_rows + rounded(partial_value)
        expert_rows = rounded(expert_rows).reshape(N_EP, CAP, D)
        placed = jnp.einsum('scn,scd->snd', picker, expert_rows).reshape(BATCH, D)
        return (running + placed * weight[:, None], None)
    expert_sum = lax.scan(expert_step, jnp.zeros((BATCH, D), jnp.float32), (jnp.arange(EXPERTS, dtype=jnp.int32), w_exp_gate, w_exp_up, w_exp_down))[0]
    return (residual_f + expert_sum + dense_out).astype(jnp.bfloat16)
```

```python
import jax
import jax.numpy as jnp
from jax import lax
from jax.sharding import Mesh
from jax.sharding import PartitionSpec as P

EP = ("ep_0", "ep_1", "ep_2")
FAR = ("ep_0", "ep_1")


EPSILON = 1e-06


def from_everyone(x, axis):
    count = lax.axis_size(axis)
    return lax.all_to_all(jnp.broadcast_to(x[None], (count, *x.shape)), axis, 0, 0, tiled=True)


def taken_together(x, axis):
    return from_everyone(x, axis).astype(jnp.float32).sum(axis=0)


def in_order(parts, dim):
    shape = list(parts.shape[1:])
    shape[dim] *= parts.shape[0]
    return jnp.moveaxis(parts, 0, dim).reshape(shape)


def whole_of(x, axes, dim):
    far, near = axes
    parts = from_everyone(from_everyone(x, far), near)
    return in_order(parts.swapaxes(0, 1).reshape(-1, *x.shape), dim)


def in_blocks(x, dim, count):
    shape = x.shape
    parts = x.reshape(*shape[:dim], count, shape[dim] // count, *shape[dim + 1 :])
    return jnp.moveaxis(parts, dim, 0)


def sent_and_summed(x, axis, dim):
    count = lax.axis_size(axis)
    parts = lax.all_to_all(in_blocks(x, dim, count), axis, 0, 0, tiled=True)
    return jnp.sum(parts.astype(jnp.float32), axis=0)


def sum_in_two_steps(x, axes, dim):
    far, near = axes
    parts = in_blocks(x, dim, lax.axis_size(far))
    nearer = sent_and_summed(parts, near, dim + 1)
    arrived = lax.all_to_all(
        nearer.astype(jnp.bfloat16), far, split_axis=0, concat_axis=0, tiled=True
    )
    return arrived.astype(jnp.float32).sum(axis=0)


def rms_scale(values, gain_row):
    mean_square = jnp.mean(values * values, axis=-1, keepdims=True)
    return values * lax.rsqrt(mean_square + EPSILON) * gain_row


def shards(
    tokens,
    attn_gain,
    w_query,
    w_key,
    w_value,
    w_forget,
    forget_bias,
    query_gain,
    key_gain,
    cache_pairs,
    cache_cum,
    lengths,
    w_output,
    ffn_gain,
    expert_ids,
    route_weight,
    w_exp_gate,
    w_exp_up,
    w_exp_down,
    shared_gate,
    w_dense_gate,
    w_dense_up,
    w_dense_down,
):
    def other(w):
        return lax.ppermute(w, "ep_2", [(0, 1), (1, 0)])

    gate_other, up_other, down_other = other(w_exp_gate[0]), other(w_exp_up[0]), other(w_exp_down[0])
    dense_gate_other, dense_up_other, dense_down_other = other(w_dense_gate), other(w_dense_up), other(w_dense_down)
    seq_rows, width = tokens.shape
    head_size = query_gain.shape[0]
    kv_here = cache_pairs.shape[1]
    cache_len = cache_pairs.shape[2]
    tokens_f = tokens.astype(jnp.float32)
    normed = rms_scale(tokens_f, attn_gain).astype(jnp.bfloat16)
    query_raw = jnp.dot(normed, w_query, preferred_element_type=jnp.float32)
    heads_here = query_raw.shape[1] // head_size
    group_size = heads_here // kv_here
    query_rows = rms_scale(
        query_raw.reshape(seq_rows, kv_here, group_size, head_size), query_gain
    ).astype(jnp.bfloat16)
    key_raw = jnp.dot(normed, w_key, preferred_element_type=jnp.float32).reshape(
        seq_rows, kv_here, head_size
    )
    fresh_key = rms_scale(key_raw, key_gain).astype(jnp.bfloat16)
    value_new = jnp.dot(normed, w_value, preferred_element_type=jnp.float32).astype(jnp.bfloat16)
    value_new = value_new.reshape(seq_rows, kv_here, head_size)
    log_gate = jax.nn.log_sigmoid(
        jnp.dot(normed, w_forget, preferred_element_type=jnp.float32) + forget_bias
    )
    position = lax.broadcasted_iota(jnp.int32, (1, 1, cache_len), 2)
    is_live = position < lengths[:, None, None]
    last_cum = jnp.sum(jnp.where(position == lengths[:, None, None] - 1, cache_cum, 0.0), axis=2)
    now_cum = last_cum + log_gate
    cached_keys = cache_pairs[..., :head_size]
    cached_values = cache_pairs[..., head_size:]
    score_multiplier = head_size ** (-0.5)
    past_score = (
        jnp.einsum("bkgd,bkld->bkgl", query_rows, cached_keys, preferred_element_type=jnp.float32)
        * score_multiplier
    )
    past_score = past_score + (now_cum[:, :, None] - cache_cum)[:, :, None, :]
    past_score = jnp.where(is_live[:, :, None, :], past_score, -jnp.inf)
    current_score = (
        jnp.einsum("nlte,nle->nlt", query_rows, fresh_key, preferred_element_type=jnp.float32)
        * score_multiplier
    )
    row_peak = jnp.maximum(jnp.max(past_score, axis=3), current_score)
    past_exp = jnp.exp(past_score - row_peak[..., None])
    own_exp = jnp.exp(current_score - row_peak)
    denom_sum = jnp.sum(past_exp, axis=3) + own_exp
    past_prob = (past_exp / denom_sum[..., None]).astype(jnp.bfloat16)
    own_prob = (own_exp / denom_sum).astype(jnp.bfloat16)
    head_mix = jnp.einsum(
        "bkgl,bkld->bkgd", past_prob, cached_values, preferred_element_type=jnp.float32
    )
    head_mix = head_mix + own_prob[..., None].astype(jnp.float32) * value_new[:, :, None, :].astype(
        jnp.float32
    )
    head_mix = head_mix.astype(jnp.bfloat16).reshape(seq_rows, heads_here * head_size)
    partial_value = jnp.dot(head_mix, w_output, preferred_element_type=jnp.float32)
    attn_out = taken_together(partial_value.astype(jnp.bfloat16), "tp").astype(jnp.float32)
    residual = (tokens_f + attn_out).astype(jnp.bfloat16)
    residual_f = residual.astype(jnp.float32)
    normed_two = rms_scale(residual_f, ffn_gain).astype(jnp.bfloat16)

    tp_at, core_at = lax.axis_index("tp"), lax.axis_index("ep_2")
    n_tp, n_core = lax.axis_size("tp"), lax.axis_size("ep_2")
    chips = lax.axis_size(FAR)
    chip_at = lax.axis_index(FAR)
    cap = 2
    share = seq_rows // n_tp

    ids = expert_ids.reshape(chips, n_core, seq_rows, -1)
    ids_plane = lax.dynamic_index_in_dim(ids, core_at, 1, keepdims=False)
    ids_own = lax.dynamic_index_in_dim(ids_plane, chip_at, 0, keepdims=False)
    cores = jnp.stack([core_at, 1 - core_at])
    dest = jnp.arange(chips)[:, None] * n_core + cores[None, :]
    hit = jnp.any(ids_own[None, None] == dest[:, :, None, None], axis=3)
    rank = jnp.cumsum(hit.astype(jnp.int32), axis=2)
    slot = jnp.arange(1, cap + 1)
    pick = (hit[:, :, None, :] & (rank[:, :, None, :] == slot[None, None, :, None])).astype(jnp.bfloat16)
    sent = jnp.dot(
        pick.reshape(-1, seq_rows), normed_two, preferred_element_type=jnp.float32
    ).astype(jnp.bfloat16)
    slots = n_core * cap
    mine = lax.dynamic_slice_in_dim(normed_two, tp_at * share, share, 0)
    message = jnp.concatenate(
        [
            sent.reshape(chips, slots, width),
            jnp.broadcast_to(mine[None], (chips, share, width)),
        ],
        axis=1,
    )
    message = message.reshape(chips, -1, 128)
    arrived = lax.all_to_all(message, FAR, 0, 0, tiled=True)
    arrived = arrived.reshape(chips, slots + share, width)
    to_expert = arrived[:, :slots].reshape(chips, n_core, cap, width)
    to_dense = arrived[:, slots:].reshape(chips * share, width)

    def expert(rows, gate_w, up_w, down_w):
        gate_part = jnp.dot(rows, gate_w, preferred_element_type=jnp.float32)
        up_part = jnp.dot(rows, up_w, preferred_element_type=jnp.float32)
        hidden = (jax.nn.silu(gate_part) * up_part).astype(jnp.bfloat16)
        return jnp.dot(hidden, down_w, preferred_element_type=jnp.float32).astype(jnp.bfloat16)

    part_own = expert(to_expert[:, 0].reshape(-1, width), w_exp_gate[0], w_exp_up[0], w_exp_down[0])
    part_other = expert(to_expert[:, 1].reshape(-1, width), gate_other, up_other, down_other)
    expert_part = jnp.stack(
        [part_own.reshape(chips, cap, width), part_other.reshape(chips, cap, width)], axis=1
    ).reshape(chips * slots, width)

    contract = (((1,), (1,)), ((), ()))
    dense_gate_w = jnp.concatenate([w_dense_gate, dense_gate_other], axis=0)
    dense_up_w = jnp.concatenate([w_dense_up, dense_up_other], axis=0)
    dense_down_w = jnp.concatenate([w_dense_down, dense_down_other], axis=0)
    dense_gate_raw = lax.dot_general(to_dense, dense_gate_w, contract, preferred_element_type=jnp.float32)
    dense_up_raw = lax.dot_general(to_dense, dense_up_w, contract, preferred_element_type=jnp.float32)
    mix_gate = jax.nn.sigmoid(jnp.dot(to_dense, shared_gate, preferred_element_type=jnp.float32))
    dense_hidden = (mix_gate[:, None] * (jax.nn.silu(dense_gate_raw) * dense_up_raw)).astype(jnp.bfloat16)
    span = width // n_tp
    hidden_size = dense_hidden.shape[1]
    blocks = jnp.concatenate(
        [
            in_blocks(expert_part, 1, n_tp),
            jnp.broadcast_to(dense_hidden.reshape(1, -1, span), (n_tp, dense_hidden.size // span, span)),
        ],
        axis=1,
    )
    crossed = lax.all_to_all(blocks, "tp", 0, 0, tiled=True)
    expert_rows = crossed[:, : chips * slots].astype(jnp.float32).sum(axis=0).astype(jnp.bfloat16)
    hidden_all = crossed[:, chips * slots :].reshape(n_tp, chips, share, hidden_size)
    hidden_all = hidden_all.swapaxes(0, 1).reshape(chips * seq_rows, hidden_size)
    dense_rows = jnp.dot(hidden_all, dense_down_w, preferred_element_type=jnp.float32)

    weights_plane = lax.dynamic_index_in_dim(
        route_weight.reshape(chips, n_core, seq_rows, -1), core_at, 1, keepdims=False
    )
    here = chip_at * n_core + cores
    chosen = ids_plane[:, None] == here[None, :, None, None]
    hit_here = jnp.any(chosen, axis=3)
    weight_here = jnp.sum(jnp.where(chosen, weights_plane[:, None], 0.0), axis=3)
    rank_here = jnp.cumsum(hit_here.astype(jnp.int32), axis=2)
    place = hit_here[:, :, None, :] & (rank_here[:, :, None, :] == slot[None, None, :, None])
    place = jnp.where(place, weight_here[:, :, None, :], 0.0).reshape(chips, slots, seq_rows)
    expert_term = jnp.einsum(
        "scn,scd->snd",
        place,
        expert_rows.reshape(chips, slots, span).astype(jnp.float32),
        precision=lax.Precision.HIGHEST,
        preferred_element_type=jnp.float32,
    )
    total = (dense_rows.reshape(chips, seq_rows, span) + expert_term).astype(jnp.bfloat16)
    summed = lax.all_to_all(total, FAR, 0, 0, tiled=True).astype(jnp.float32).sum(axis=0)
    own_residual = lax.dynamic_slice_in_dim(residual_f, tp_at * span, span, 1)
    return (own_residual + summed).astype(jnp.bfloat16)


def solution(mesh):
    split = Mesh(mesh.devices.reshape(8, 4, 2, mesh.shape["tp"]), ("ep_0", "ep_1", "ep_2", "tp"))
    return jax.shard_map(
        shards,
        mesh=split,
        in_specs=(
            P(EP, None),
            P(),
            P(None, "tp"),
            P(None, "tp"),
            P(None, "tp"),
            P(None, "tp"),
            P("tp"),
            P(),
            P(),
            P(EP, "tp", None, None),
            P(EP, "tp", None),
            P(EP),
            P("tp", None),
            P(),
            P(),
            P(),
            P(EP, None, "tp"),
            P(EP, None, "tp"),
            P(EP, "tp", None),
            P(),
            P(EP, None),
            P(EP, None),
            P(EP, "tp"),
        ),
        out_specs=P(EP, "tp"),
        check_vma=False,
    )
```

```python
import functools

import jax
import jax.numpy as jnp
from jax import lax
from jax.experimental import pallas as pl
from jax.experimental.pallas import tpu as pltpu
from jax.sharding import Mesh
from jax.sharding import PartitionSpec as P

EP = ("ep_0", "ep_1", "ep_2")
FAR = ("ep_0", "ep_1")
EPSILON = 1e-06
F32, BF16 = jnp.float32, jnp.bfloat16
CAP = 2
LANES = 128
MIB = 1 << 20
ANY = pl.BlockSpec(memory_space=pl.ANY)
IN_VMEM = pl.BlockSpec(memory_space=pltpu.VMEM)
IN_SMEM = pl.BlockSpec(memory_space=pltpu.SMEM)
NT = (((1,), (1,)), ((), ()))


def at_hbm(x):
    return pltpu.with_memory_space_constraint(x, pltpu.HBM)


def at_vmem(x):
    return pltpu.with_memory_space_constraint(x, pltpu.VMEM)


def normal_rows(values, gain_row):
    mean_square = jnp.mean(values * values, axis=-1, keepdims=True)
    return values * lax.rsqrt(mean_square + EPSILON) * gain_row


def dot(a, b):
    return jnp.dot(a, b, preferred_element_type=F32)


def dot_nt(a, b):
    return lax.dot_general(a, b, NT, preferred_element_type=F32)


def rows_of(shape):
    return lax.broadcasted_iota(jnp.int32, shape, 0)


def lanes_of(shape):
    return lax.broadcasted_iota(jnp.int32, shape, 1)


def route_tables(ids, weights, taken_ref, place_ref):
    n_tp, n_core = lax.axis_size("tp"), lax.axis_size("ep_2")
    core_at, chip_at = lax.axis_index("ep_2"), lax.axis_index(FAR)
    rows, wide = taken_ref.shape[1:]
    batch = ids.shape[1]
    seqs = wide // n_tp
    cores = (core_at, 1 - core_at)
    ids = ids[...]

    lane = lanes_of((wide, batch))
    own = lane == (chip_at * n_core + core_at) * seqs + rows_of((wide, batch)) % seqs
    own = jnp.where(own, 1.0, 0.0).astype(BF16)
    padded = jnp.concatenate([ids.astype(F32), jnp.zeros((6, batch), F32)], axis=0).astype(BF16)
    own_ids = dot_nt(padded, own).astype(jnp.int32)
    row, lane = rows_of((rows, wide)), lanes_of((rows, wide))
    piece_fits = lane // seqs == row % n_tp
    slot = (row % (2 * n_tp)) // n_tp
    first, second = rows_of((wide, wide)), lanes_of((wide, wide))
    ahead = (first // seqs == second // seqs) & (first <= second)
    ahead = jnp.where(ahead, 1.0, 0.0).astype(BF16)
    for o in range(2):
        expert = (row // (2 * n_tp)) * n_core + cores[o]
        hit = (expert == own_ids[0:1, :]) | (expert == own_ids[1:2, :])
        rank = dot(jnp.where(hit, 1.0, 0.0).astype(BF16), ahead).astype(jnp.int32)
        taken = hit & (rank == slot + 1) & piece_fits
        taken_ref[o] = jnp.where(taken, 1.0, 0.0).astype(BF16)

    half = place_ref.shape[2] // 2
    lane = lanes_of((1, batch))
    in_plane = (lane // seqs) % n_core == core_at
    mine = lanes_of((seqs, batch)) % seqs == rows_of((seqs, batch))
    stacked = []
    for o in range(2):
        expert = chip_at * n_core + cores[o]
        hits = (ids == expert) & in_plane
        weight = jnp.sum(jnp.where(hits, weights[...], 0.0), axis=0, keepdims=True)
        high = weight.astype(BF16).astype(F32)
        hit = jnp.sum(jnp.where(hits, 1.0, 0.0), axis=0, keepdims=True)
        stacked += [jnp.where(mine, part, 0.0) for part in (hit, high, weight - high)]
    stacked = jnp.concatenate(stacked, axis=0).astype(BF16)
    group = lanes_of((half, batch)) // (seqs * n_core) == rows_of((half, batch)) // CAP
    table = dot_nt(stacked, jnp.where(group, 1.0, 0.0).astype(BF16))
    before = rows_of((seqs, seqs)) >= lanes_of((seqs, seqs))
    before = jnp.where(before, 1.0, 0.0).astype(BF16)
    slot = lanes_of((seqs, half)) % CAP + 1
    for o in range(2):
        hit, high, low = (table[(3 * o + i) * seqs : (3 * o + i + 1) * seqs] for i in range(3))
        rank = dot(before, hit.astype(BF16)).astype(jnp.int32)
        put = (hit > 0.5) & (rank == slot)
        place_ref[0, :, o * half : (o + 1) * half] = jnp.where(put, high, 0.0).astype(BF16)
        place_ref[1, :, o * half : (o + 1) * half] = jnp.where(put, low, 0.0).astype(BF16)


def attend_kernel(chunks, lens, forget_bias, *refs):
    sources, (out_ref, taken_ref, place_ref), rest = refs[:13], refs[13:16], refs[16:]
    held, (queries, keys, values, shift, scores, mixed, sems) = rest[:13], rest[13:]
    ids, weights, tok, gain, wq, wk, wv, wf, qg, kg, cum, wo, cache = held
    seqs, slots, pair = cache.shape
    head = qg.shape[1]
    group = wq.shape[1] // head
    copies = [pltpu.make_async_copy(sources[i], held[i], sems.at[i]) for i in range(12)]
    step = seqs // chunks
    parts = [
        pltpu.make_async_copy(
            sources[12].at[pl.ds(i * step, step)], cache.at[pl.ds(i * step, step)], sems.at[12 + i]
        )
        for i in range(chunks)
    ]
    for copy in copies[:11]:
        copy.start()
    for part in parts:
        part.start()
    copies[11].start()
    for copy in copies[:2]:
        copy.wait()
    route_tables(ids, weights, taken_ref, place_ref)
    for copy in copies[2:10]:
        copy.wait()

    normed = normal_rows(tok[...].astype(F32), gain[...]).astype(BF16)
    query_raw = dot(normed, wq[...])
    key_new = normal_rows(dot_nt(normed, wk[...]), kg[...]).astype(BF16).astype(F32)
    value_new = dot_nt(normed, wv[...]).astype(BF16).astype(F32)
    blank = jnp.zeros((seqs, pair - head), F32)
    key_new = jnp.concatenate([key_new, blank], axis=1)
    value_new = jnp.concatenate([blank, value_new], axis=1)
    for h in range(group):
        query = normal_rows(query_raw[:, h * head : (h + 1) * head], qg[...])
        query = jnp.concatenate([query.astype(BF16).astype(F32), blank], axis=1)
        queries[pl.ds(h, seqs, stride=group), :] = query
        keys[pl.ds(h, seqs, stride=group), :] = key_new
        values[pl.ds(h, seqs, stride=group), :] = value_new
    forget = jnp.sum(normed.astype(F32) * wf[...].astype(F32), axis=1, keepdims=True) + forget_bias[0]
    log_gate = jnp.minimum(forget, 0.0) - jnp.log1p(jnp.exp(-jnp.abs(forget)))

    row = rows_of((seqs, 1))
    length = jnp.zeros((seqs, 1), jnp.int32)
    for s in range(seqs):
        length = jnp.where(row == s, lens[s], length)
    copies[10].wait()
    position = lanes_of((seqs, slots))
    summed = cum[...].reshape(seqs, slots)
    last = jnp.sum(jnp.where(position == length - 1, summed, 0.0), axis=1, keepdims=True)
    shift[...] = jnp.where(position < length, (last + log_gate) - summed, -jnp.inf)

    multiplier = head ** (-0.5)
    own_score = jnp.sum(queries[...] * keys[...], axis=1, keepdims=True) * multiplier
    tall = 2 * group
    upper = rows_of((tall, 1)) < group
    for p in range(seqs // 2):
        if (2 * p) % step == 0:
            parts[2 * p // step].wait()
        query = queries[tall * p : tall * (p + 1), :].astype(BF16)
        score = jnp.where(upper, dot_nt(query, cache[2 * p]), dot_nt(query, cache[2 * p + 1]))
        moved = jnp.where(upper, shift[2 * p : 2 * p + 1, :], shift[2 * p + 1 : 2 * p + 2, :])
        scores[tall * p : tall * (p + 1), :] = score * multiplier + moved
    score = scores[...]
    peak = jnp.maximum(jnp.max(score, axis=1, keepdims=True), own_score)
    past = jnp.exp(score - peak)
    own = jnp.exp(own_score - peak)
    whole = 1.0 / (jnp.sum(past, axis=1, keepdims=True) + own)
    scores[...] = past * whole
    own_prob = (own * whole).astype(BF16).astype(F32)
    for p in range(seqs // 2):
        prob = scores[tall * p : tall * (p + 1), :].astype(BF16)
        mixed[tall * p : tall * (p + 1), :] = jnp.where(
            upper, dot(prob, cache[2 * p]), dot(prob, cache[2 * p + 1])
        )
    mixed[...] = mixed[...] + own_prob * values[...]
    copies[11].wait()
    total = jnp.zeros((seqs, wo.shape[1]), F32)
    for h in range(group):
        mix = mixed[pl.ds(h, seqs, stride=group), :][:, pair - head :].astype(BF16)
        total = total + dot(mix, wo[h * head : (h + 1) * head, :])
    partial = total.astype(BF16)
    for t in range(out_ref.shape[0]):
        out_ref[t] = partial


def attend(n_tp, chips, lens, forget_bias, *arrays):
    chunks = 6
    tok, wq, qg, cache = arrays[2], arrays[4], arrays[8], arrays[12]
    seqs, slots, pair = cache.shape
    heads = wq.shape[1] // qg.shape[1]
    rows = seqs * heads
    scratch = [pltpu.VMEM(a.shape, a.dtype) for a in arrays]
    scratch += [pltpu.VMEM((rows, pair), F32)] * 3
    scratch += [pltpu.VMEM((seqs, slots), F32), pltpu.VMEM((rows, slots), F32), pltpu.VMEM((rows, pair), F32)]
    scratch += [pltpu.SemaphoreType.DMA((12 + chunks,))]
    return pl.pallas_call(
        functools.partial(attend_kernel, chunks),
        name="attend",
        out_shape=(
            pltpu.VMEM((n_tp, *tok.shape), BF16),
            pltpu.VMEM((2, chips * 2 * n_tp, n_tp * seqs), BF16),
            pltpu.VMEM((2, seqs, chips * 2 * CAP), BF16),
        ),
        in_specs=[IN_SMEM, IN_SMEM] + [ANY] * 13,
        out_specs=(IN_VMEM,) * 3,
        scratch_shapes=scratch,
        compiler_params=pltpu.CompilerParams(vmem_limit_bytes=16 * MIB),
    )(lens, forget_bias, *[at_hbm(a) for a in arrays])


def send_kernel(crossed, tok, gain, taken_ref, *refs):
    message, own_residual = refs[-2:]
    n_tp = crossed.shape[0]
    seqs, width = tok.shape
    rows = message.shape[0]
    span = width // n_tp
    share = seqs // n_tp
    tp_at = lax.axis_index("tp")
    attn_out = crossed[0].astype(F32)
    for t in range(1, n_tp):
        attn_out = attn_out + crossed[t].astype(F32)
    residual = (tok[...].astype(F32) + attn_out).astype(BF16)
    residual_f = residual.astype(F32)
    kept = residual[:, :span]
    for t in range(1, n_tp):
        kept = jnp.where(tp_at == t, residual[:, t * span : (t + 1) * span], kept)
    own_residual[...] = kept
    normed = normal_rows(residual_f, gain[...])
    pieces = jnp.concatenate([normed[:, q * span : (q + 1) * span] for q in range(n_tp)], axis=0)
    pieces = pieces.astype(BF16)
    wide = n_tp * seqs
    for o in range(2):
        message[:, o * span : (o + 1) * span] = dot(taken_ref[o], pieces).astype(BF16)
    each = 2 * n_tp
    row, lane = rows_of((each, wide)), lanes_of((each, wide))
    for two in range(share // 2):
        token = tp_at * share + two * 2 + row // n_tp
        taken = (lane // seqs == row % n_tp) & (lane % seqs == token)
        block = dot(jnp.where(taken, 1.0, 0.0).astype(BF16), pieces).astype(BF16)
        block = jnp.broadcast_to(block[None], (rows // each, each, span)).reshape(rows, span)
        message[:, (2 + two) * span : (3 + two) * span] = block


def send(crossed, tok, gain, taken, chips, swapped):
    n_tp, seqs, width = crossed.shape
    span = width // n_tp
    rows = chips * 2 * n_tp
    return pl.pallas_call(
        send_kernel,
        name="send",
        out_shape=(
            pltpu.VMEM((rows, (2 + seqs // n_tp // 2) * span), BF16),
            pltpu.VMEM((seqs, span), BF16),
        ),
        in_specs=[IN_VMEM] * 4 + [ANY] * len(swapped),
        out_specs=(IN_VMEM, IN_VMEM),
        compiler_params=pltpu.CompilerParams(vmem_limit_bytes=8 * MIB),
    )(at_vmem(crossed), tok, gain, at_vmem(taken), *[at_hbm(w) for w in swapped])


def experts_kernel(n_tp, arrived, shared, *refs):
    weights, out_ref, spread, held, sems = refs[:10], refs[10], refs[11], refs[12:-1], refs[-1]
    matrices, (dense_gate, dense_up) = held[:6], held[6:]
    units = weights[6].shape[0]
    into = (dense_gate.at[:units], dense_gate.at[units:], dense_up.at[:units], dense_up.at[units:])
    into = matrices + into
    copies = [pltpu.make_async_copy(weights[i], into[i], sems.at[i]) for i in range(10)]
    for copy in copies[6:] + copies[:6]:
        copy.start()
    rows, span = arrived.shape[0], out_ref.shape[2]
    each = 2 * n_tp
    chips = rows // each
    for j in range(spread.shape[0]):
        spread[j] = arrived[:, j * LANES : (j + 1) * LANES].astype(F32)

    def gathered(start, stride, count, column):
        return jnp.concatenate(
            [
                spread[column // LANES + j, pl.ds(start + q, count, stride=stride), :]
                for q in range(n_tp)
                for j in range(span // LANES)
            ],
            axis=1,
        )

    blocks = []
    for two in range(arrived.shape[1] // span - 2):
        for k in range(2):
            blocks.append(gathered(k * n_tp, each, chips, (2 + two) * span))
    tokens = jnp.concatenate(blocks, axis=0).astype(BF16)
    gate_row = shared[...].astype(F32)
    gate_row = jnp.concatenate([gate_row[i : i + 1] for i in range(gate_row.shape[0])], axis=1)
    gate_rows = jnp.broadcast_to(gate_row, (8, gate_row.shape[1])).astype(BF16)
    mix_gate = dot_nt(tokens, gate_rows)[:, :1]
    mix_gate = 1.0 / (1.0 + jnp.exp(-mix_gate))
    for copy in copies[6:]:
        copy.wait()
    gate = dot_nt(tokens, dense_gate[...])
    up = dot_nt(tokens, dense_up[...])
    hidden = (mix_gate * (gate / (1.0 + jnp.exp(-gate)) * up)).astype(BF16)
    half = hidden.shape[0] // 2
    taken = chips * 2 * CAP
    for t in range(n_tp):
        out_ref[t, taken:, : span // 2] = hidden[:half]
        out_ref[t, taken:, span // 2 :] = hidden[half:]
    for o in range(2):
        tokens = gathered(0, n_tp, chips * CAP, o * span).astype(BF16)
        gate_w, up_w, down_w = matrices[3 * o : 3 * o + 3]
        copies[3 * o].wait()
        gate = dot(tokens, gate_w[...])
        copies[3 * o + 1].wait()
        up = dot(tokens, up_w[...])
        hidden = (gate / (1.0 + jnp.exp(-gate)) * up).astype(BF16)
        copies[3 * o + 2].wait()
        part = dot(hidden, down_w[...]).astype(BF16)
        for t in range(n_tp):
            out_ref[t, o * chips * CAP : (o + 1) * chips * CAP, :] = part[:, t * span : (t + 1) * span]


def experts(n_tp, span, arrived, shared, matrices, dense):
    rows = arrived.shape[0]
    chips = rows // (2 * n_tp)
    many = (arrived.shape[1] // span - 2) * 2 * chips
    units, width = dense[0].shape
    return pl.pallas_call(
        functools.partial(experts_kernel, n_tp),
        name="experts",
        out_shape=pltpu.VMEM((n_tp, chips * 2 * CAP + many // 2, span), BF16),
        in_specs=[IN_VMEM] * 2 + [ANY] * 10,
        out_specs=IN_VMEM,
        scratch_shapes=[pltpu.VMEM((arrived.shape[1] // LANES, rows, LANES), F32)]
        + [pltpu.VMEM(w.shape, w.dtype) for w in matrices]
        + [pltpu.VMEM((2 * units, width), BF16)] * 2
        + [pltpu.SemaphoreType.DMA((10,))],
        compiler_params=pltpu.CompilerParams(vmem_limit_bytes=24 * MIB),
    )(at_vmem(arrived), shared, *[at_hbm(w) for w in matrices], *[at_hbm(w) for w in dense])


def combine_kernel(crossed, place, down_own, down_other, out_ref, dense):
    n_tp, _, span = crossed.shape
    chips, seqs, _ = out_ref.shape
    taken = chips * 2 * CAP
    share = seqs // n_tp
    total = crossed[0, :taken].astype(F32)
    for t in range(1, n_tp):
        total = total + crossed[t, :taken].astype(F32)
    total = total.astype(BF16)
    down = jnp.concatenate([down_own[...], down_other[...]], axis=0)
    for t in range(n_tp):
        both = crossed[t, taken:]
        hidden = jnp.concatenate([both[:, : span // 2], both[:, span // 2 :]], axis=0)
        part = dot(hidden, down)
        for c in range(share):
            for j in range(dense.shape[0]):
                dense[j, pl.ds(t * share + c, chips, stride=seqs), :] = part[
                    c * chips : (c + 1) * chips, j * LANES : (j + 1) * LANES
                ]
    lane = lanes_of((seqs, taken))
    owner = (lane % (chips * CAP)) // CAP
    spread = jnp.zeros((chips * seqs, span), F32)
    for i in range(2):
        weight = place[i].astype(F32)
        weight = jnp.concatenate([jnp.where(owner == s, weight, 0.0) for s in range(chips)], axis=0)
        spread = spread + dot(weight.astype(BF16), total)
    for j in range(dense.shape[0]):
        column = spread[:, j * LANES : (j + 1) * LANES]
        out_ref[:, :, j * LANES : (j + 1) * LANES] = (dense[j] + column).astype(BF16).reshape(chips, seqs, LANES)


def combine(crossed, place, down_own, down_other, chips, seqs):
    span = crossed.shape[2]
    return pl.pallas_call(
        combine_kernel,
        name="combine",
        out_shape=pltpu.VMEM((chips, seqs, span), BF16),
        in_specs=[IN_VMEM] * 4,
        out_specs=IN_VMEM,
        scratch_shapes=[pltpu.VMEM((span // LANES, chips * seqs, LANES), F32)],
        compiler_params=pltpu.CompilerParams(vmem_limit_bytes=8 * MIB),
    )(at_vmem(crossed), at_vmem(place), at_vmem(down_own), at_vmem(down_other))


def shards(
    tokens,
    attn_gain,
    w_query,
    w_key,
    w_value,
    w_forget,
    forget_bias,
    query_gain,
    key_gain,
    cache_pairs,
    cache_cum,
    lengths,
    w_output,
    ffn_gain,
    expert_ids,
    route_weight,
    w_exp_gate,
    w_exp_up,
    w_exp_down,
    shared_gate,
    w_dense_gate,
    w_dense_up,
    w_dense_down,
):
    seqs, width = tokens.shape
    n_tp, chips = lax.axis_size("tp"), lax.axis_size(FAR)
    span = width // n_tp

    def other(w):
        return lax.ppermute(w, "ep_2", [(0, 1), (1, 0)])

    matrices = [w_exp_gate[0], w_exp_up[0], w_exp_down[0]]
    matrices = matrices + [other(w) for w in matrices]
    dense = [w_dense_gate, other(w_dense_gate), w_dense_up, other(w_dense_up)]
    down_other = other(w_dense_down)

    partial, taken, place = attend(
        n_tp,
        chips,
        lengths,
        forget_bias,
        expert_ids.T,
        route_weight.T,
        tokens,
        attn_gain[None],
        w_query,
        w_key.T,
        w_value.T,
        w_forget.T,
        query_gain[None],
        key_gain[None],
        cache_cum,
        w_output,
        cache_pairs[:, 0],
    )
    crossed = lax.all_to_all(partial, "tp", 0, 0, tiled=True)
    message, own_residual = send(
        crossed, tokens, ffn_gain[None], taken, chips, [*matrices[3:], dense[1], dense[3], down_other]
    )
    arrived = lax.all_to_all(message.reshape(chips, -1, message.shape[1]), FAR, 0, 0, tiled=True)
    blocks = experts(n_tp, span, arrived.reshape(message.shape), shared_gate.reshape(-1, LANES), matrices, dense)
    crossed = lax.all_to_all(blocks, "tp", 0, 0, tiled=True)
    total = combine(crossed, place, w_dense_down, down_other, chips, seqs)
    summed = lax.all_to_all(total, FAR, 0, 0, tiled=True).astype(F32).sum(axis=0)
    return (own_residual.astype(F32) + summed).astype(BF16)


def solution(mesh):
    split = Mesh(mesh.devices.reshape(8, 4, 2, mesh.shape["tp"]), ("ep_0", "ep_1", "ep_2", "tp"))
    return jax.shard_map(
        shards,
        mesh=split,
        in_specs=(
            P(EP, None),
            P(),
            P(None, "tp"),
            P(None, "tp"),
            P(None, "tp"),
            P(None, "tp"),
            P("tp"),
            P(),
            P(),
            P(EP, "tp", None, None),
            P(EP, "tp", None),
            P(EP),
            P("tp", None),
            P(),
            P(),
            P(),
            P(EP, None, "tp"),
            P(EP, None, "tp"),
            P(EP, "tp", None),
            P(),
            P(EP, None),
            P(EP, None),
            P(EP, "tp"),
        ),
        out_specs=P(EP, "tp"),
        check_vma=False,
    )
```

```python
import functools

import jax
import jax.numpy as jnp
from jax import lax
from jax.experimental import pallas as pl
from jax.experimental.pallas import tpu as pltpu
from jax.sharding import Mesh
from jax.sharding import PartitionSpec as P


EP = ("ep_0", "ep_1", "ep_2")
FAR = ("ep_0", "ep_1")
EPSILON = 1e-06
F32, BF16 = jnp.float32, jnp.bfloat16
CAP = 2
LANES = 128
MIB = 1 << 20
ANY = pl.BlockSpec(memory_space=pl.ANY)
IN_VMEM = pl.BlockSpec(memory_space=pltpu.VMEM)
IN_SMEM = pl.BlockSpec(memory_space=pltpu.SMEM)
NT = (((1,), (1,)), ((), ()))


def at_hbm(x):
    return pltpu.with_memory_space_constraint(x, pltpu.HBM)


def at_vmem(x):
    return pltpu.with_memory_space_constraint(x, pltpu.VMEM)


def normal_rows(values, gain_row):
    mean_square = jnp.mean(values * values, axis=-1, keepdims=True)
    return values * lax.rsqrt(mean_square + EPSILON) * gain_row


def dot(a, b):
    return jnp.dot(a, b, preferred_element_type=F32)


def dot_nt(a, b):
    return lax.dot_general(a, b, NT, preferred_element_type=F32)


def rows_of(shape):
    return lax.broadcasted_iota(jnp.int32, shape, 0)


def lanes_of(shape):
    return lax.broadcasted_iota(jnp.int32, shape, 1)


def route_tables(ids, weights, taken_ref, place_ref):
    n_tp, n_core = lax.axis_size("tp"), lax.axis_size("ep_2")
    core_at, chip_at = lax.axis_index("ep_2"), lax.axis_index(FAR)
    rows, wide = taken_ref.shape[1:]
    batch = ids.shape[1]
    seqs = wide // n_tp
    each = 2 * n_tp
    cores = (core_at, 1 - core_at)
    base = (chip_at * n_core + core_at) * seqs
    ids, weights = ids[...].astype(F32), weights[...]

    own = lanes_of((wide, batch)) == base + rows_of((wide, batch)) % seqs
    padded = jnp.concatenate([ids, jnp.zeros((6, batch), F32)], axis=0).astype(BF16)
    own_ids = dot_nt(padded, jnp.where(own, 1.0, 0.0).astype(BF16)).astype(jnp.int32)
    row, lane = rows_of((rows, wide)), lanes_of((rows, wide))
    piece_fits = lane // seqs == row % n_tp
    slot = (row % each) // n_tp
    first, second = rows_of((wide, wide)), lanes_of((wide, wide))
    ahead = (first // seqs == second // seqs) & (first <= second)
    ahead = jnp.where(ahead, 1.0, 0.0).astype(BF16)
    for o in range(2):
        expert = (row // each) * n_core + cores[o]
        hit = (expert == own_ids[0:1, :]) | (expert == own_ids[1:2, :])
        rank = dot(jnp.where(hit, 1.0, 0.0).astype(BF16), ahead).astype(jnp.int32)
        taken = hit & (rank == slot + 1) & piece_fits
        taken_ref[o] = jnp.where(taken, 1.0, 0.0).astype(BF16)

    mine = lanes_of((seqs, batch)) == base + rows_of((seqs, batch))

    def column(values):
        return jnp.sum(jnp.where(mine, values, 0.0), axis=1, keepdims=True)

    lane = lanes_of((seqs, rows))
    slot = lane % each - 2 * CAP
    expert = (lane // each) * n_core + jnp.where(slot < CAP, cores[0], cores[1])
    weight = jnp.zeros((seqs, rows), F32)
    hit = jnp.zeros((seqs, rows), F32)
    for i in range(ids.shape[0]):
        fits = column(ids[i : i + 1]).astype(jnp.int32) == expert
        weight = jnp.where(fits, column(weights[i : i + 1]), weight)
        hit = jnp.where(fits, 1.0, hit)
    before = rows_of((seqs, seqs)) >= lanes_of((seqs, seqs))
    rank = dot(jnp.where(before, 1.0, 0.0).astype(BF16), hit.astype(BF16)).astype(jnp.int32)
    put = (slot >= 0) & (hit > 0.5) & (rank == slot % CAP + 1)
    weight = jnp.where(put, weight, 0.0)
    high = weight.astype(BF16).astype(F32)

    token, place_at = rows_of((seqs, rows)), lane % each
    share = seqs // n_tp
    part = share // 2

    def fits(index):
        return token == (index // part) * share + ((lane // each) % 2) * part + index % part

    first = jnp.where(fits(place_at), 1.0, 0.0)
    second = jnp.where((place_at < 2 * CAP) & fits(place_at + each), 1.0, 0.0)
    for i, table in enumerate((first, second + high, weight - high)):
        place_ref[i] = table.astype(BF16)


def prepare_kernel(ids_hbm, weights_hbm, *refs):
    dense, (taken_ref, place_ref, packed, ids, weights, sems) = refs[:3], refs[3:]
    copies = [
        pltpu.make_async_copy(ids_hbm, ids, sems.at[0]),
        pltpu.make_async_copy(weights_hbm, weights, sems.at[1]),
    ]
    at = 0
    for i, source in enumerate(dense):
        into = packed.at[:, at : at + source.shape[1]]
        copies.append(pltpu.make_async_copy(source, into, sems.at[2 + i]))
        at += source.shape[1]
    for copy in copies:
        copy.start()
    for copy in copies[:2]:
        copy.wait()
    route_tables(ids, weights, taken_ref, place_ref)
    for copy in copies[2:]:
        copy.wait()


def prepare(n_tp, chips, seqs, ids, weights, dense):
    return pl.pallas_call(
        prepare_kernel,
        name="prepare",
        out_shape=(
            pltpu.VMEM((2, chips * 2 * n_tp, n_tp * seqs), BF16),
            pltpu.VMEM((3, seqs, chips * 2 * n_tp), BF16),
            pltpu.VMEM((dense[0].shape[0], sum(w.shape[1] for w in dense)), BF16),
        ),
        in_specs=[ANY] * 5,
        out_specs=(IN_VMEM,) * 3,
        scratch_shapes=[
            pltpu.VMEM(ids.shape, ids.dtype),
            pltpu.VMEM(weights.shape, weights.dtype),
            pltpu.SemaphoreType.DMA((5,)),
        ],
        compiler_params=pltpu.CompilerParams(vmem_limit_bytes=8 * MIB),
    )(at_hbm(ids), at_hbm(weights), *[at_hbm(w) for w in dense])


def attend_kernel(chunks, forget_bias, lens_hbm, after, *refs):
    sources, out_ref, rest = refs[:11], refs[11], refs[12:]
    held, (lens, queries, keys, values, shift, scores, mixed, sems) = rest[:11], rest[11:]
    tok, gain, wq, wk, wv, wf, qg, kg, cum, wo, cache = held
    seqs, slots, pair = cache.shape
    head = qg.shape[1]
    group = wq.shape[1] // head
    copies = [pltpu.make_async_copy(sources[i], held[i], sems.at[i]) for i in range(10)]
    step = seqs // chunks
    parts = [
        pltpu.make_async_copy(
            sources[10].at[pl.ds(i * step, step)], cache.at[pl.ds(i * step, step)], sems.at[10 + i]
        )
        for i in range(chunks)
    ]
    lens_copy = pltpu.make_async_copy(lens_hbm, lens, sems.at[10 + chunks])
    lens_copy.start()
    for copy in copies[:9]:
        copy.start()
    for part in parts:
        part.start()
    copies[9].start()
    for copy in copies[:8]:
        copy.wait()

    normed = normal_rows(tok[...].astype(F32), gain[...]).astype(BF16)
    query_raw = dot(normed, wq[...])
    key_new = normal_rows(dot_nt(normed, wk[...]), kg[...]).astype(BF16).astype(F32)
    value_new = dot_nt(normed, wv[...]).astype(BF16).astype(F32)
    blank = jnp.zeros((seqs, pair - head), F32)
    key_new = jnp.concatenate([key_new, blank], axis=1)
    value_new = jnp.concatenate([blank, value_new], axis=1)
    for h in range(group):
        query = normal_rows(query_raw[:, h * head : (h + 1) * head], qg[...])
        query = jnp.concatenate([query.astype(BF16).astype(F32), blank], axis=1)
        queries[pl.ds(h, seqs, stride=group), :] = query
        keys[pl.ds(h, seqs, stride=group), :] = key_new
        values[pl.ds(h, seqs, stride=group), :] = value_new
    forget = jnp.sum(normed.astype(F32) * wf[...].astype(F32), axis=1, keepdims=True) + forget_bias[0]
    log_gate = jnp.minimum(forget, 0.0) - jnp.log1p(jnp.exp(-jnp.abs(forget)))

    lens_copy.wait()
    row = rows_of((seqs, 1))
    length = jnp.zeros((seqs, 1), jnp.int32)
    for s in range(seqs):
        length = jnp.where(row == s, lens[s], length)
    copies[8].wait()
    position = lanes_of((seqs, slots))
    summed = cum[...].reshape(seqs, slots)
    last = jnp.sum(jnp.where(position == length - 1, summed, 0.0), axis=1, keepdims=True)
    shift[...] = jnp.where(position < length, (last + log_gate) - summed, -jnp.inf)

    multiplier = head ** (-0.5)
    own_score = jnp.sum(queries[...] * keys[...], axis=1, keepdims=True) * multiplier
    tall = 2 * group
    upper = rows_of((tall, 1)) < group
    for p in range(seqs // 2):
        if (2 * p) % step == 0:
            parts[2 * p // step].wait()
        query = queries[tall * p : tall * (p + 1), :].astype(BF16)
        score = jnp.where(upper, dot_nt(query, cache[2 * p]), dot_nt(query, cache[2 * p + 1]))
        moved = jnp.where(upper, shift[2 * p : 2 * p + 1, :], shift[2 * p + 1 : 2 * p + 2, :])
        scores[tall * p : tall * (p + 1), :] = score * multiplier + moved
    score = scores[...]
    peak = jnp.maximum(jnp.max(score, axis=1, keepdims=True), own_score)
    past = jnp.exp(score - peak)
    own = jnp.exp(own_score - peak)
    whole = 1.0 / (jnp.sum(past, axis=1, keepdims=True) + own)
    scores[...] = past * whole
    own_prob = (own * whole).astype(BF16).astype(F32)
    for p in range(seqs // 2):
        prob = scores[tall * p : tall * (p + 1), :].astype(BF16)
        mixed[tall * p : tall * (p + 1), :] = jnp.where(
            upper, dot(prob, cache[2 * p]), dot(prob, cache[2 * p + 1])
        )
    mixed[...] = mixed[...] + own_prob * values[...]
    copies[9].wait()
    total = jnp.zeros((seqs, wo.shape[1]), F32)
    for h in range(group):
        mix = mixed[pl.ds(h, seqs, stride=group), :][:, pair - head :].astype(BF16)
        total = total + dot(mix, wo[h * head : (h + 1) * head, :])
    partial = total.astype(BF16)
    for t in range(out_ref.shape[0]):
        out_ref[t] = partial


def attend(n_tp, lens, forget_bias, after, *arrays):
    chunks = 6
    tok, wq, qg, cache = arrays[0], arrays[2], arrays[6], arrays[10]
    seqs, slots, pair = cache.shape
    heads = wq.shape[1] // qg.shape[1]
    rows = seqs * heads
    scratch = [pltpu.VMEM(a.shape, a.dtype) for a in arrays]
    scratch += [pltpu.SMEM(lens.shape, lens.dtype)]
    scratch += [pltpu.VMEM((rows, pair), F32)] * 3
    scratch += [pltpu.VMEM((seqs, slots), F32), pltpu.VMEM((rows, slots), F32), pltpu.VMEM((rows, pair), F32)]
    scratch += [pltpu.SemaphoreType.DMA((11 + chunks,))]
    return pl.pallas_call(
        functools.partial(attend_kernel, chunks),
        name="attend",
        out_shape=pltpu.VMEM((n_tp, *tok.shape), BF16),
        in_specs=[IN_SMEM] + [ANY] * 13,
        out_specs=IN_VMEM,
        scratch_shapes=scratch,
        compiler_params=pltpu.CompilerParams(vmem_limit_bytes=16 * MIB),
    )(forget_bias, at_hbm(lens), after, *[at_hbm(a) for a in arrays])


def send_kernel(crossed, tok, gain, taken_ref, *refs):
    message, own_residual = refs[-2:]
    n_tp = crossed.shape[0]
    seqs, width = tok.shape
    rows = message.shape[0]
    span = width // n_tp
    share = seqs // n_tp
    tp_at = lax.axis_index("tp")
    attn_out = crossed[0].astype(F32)
    for t in range(1, n_tp):
        attn_out = attn_out + crossed[t].astype(F32)
    residual = (tok[...].astype(F32) + attn_out).astype(BF16)
    residual_f = residual.astype(F32)
    kept = residual[:, :span]
    for t in range(1, n_tp):
        kept = jnp.where(tp_at == t, residual[:, t * span : (t + 1) * span], kept)
    own_residual[...] = kept
    normed = normal_rows(residual_f, gain[...])
    pieces = jnp.concatenate([normed[:, q * span : (q + 1) * span] for q in range(n_tp)], axis=0)
    pieces = pieces.astype(BF16)
    wide = n_tp * seqs
    for o in range(2):
        message[:, o * span : (o + 1) * span] = dot(taken_ref[o], pieces).astype(BF16)
    each = 2 * n_tp
    both = 2 * each
    part = share // 2
    narrow = span // 2
    row, lane = rows_of((both, wide)), lanes_of((both, wide))
    token = tp_at * share + (row // each) * part + (row % each) // n_tp
    fits = (lane // seqs == row % n_tp) & (lane % seqs == token)
    block = dot(jnp.where(fits, 1.0, 0.0).astype(BF16), pieces).astype(BF16)
    block = jnp.broadcast_to(block[None], (rows // both, both, span)).reshape(rows, span)
    message[:, 2 * span : 3 * span] = block
    pieces = jnp.concatenate([normed[:, q * narrow : (q + 1) * narrow] for q in range(each)], axis=0)
    row, lane = rows_of((both, each * seqs)), lanes_of((both, each * seqs))
    token = tp_at * share + (row // each) * part + part - 1
    fits = (lane // seqs == row % each) & (lane % seqs == token)
    block = dot(jnp.where(fits, 1.0, 0.0).astype(BF16), pieces.astype(BF16)).astype(BF16)
    block = jnp.broadcast_to(block[None], (rows // both, both, narrow)).reshape(rows, narrow)
    message[:, 3 * span :] = block


def send(crossed, tok, gain, taken, chips, swapped):
    n_tp, seqs, width = crossed.shape
    span = width // n_tp
    rows = chips * 2 * n_tp
    return pl.pallas_call(
        send_kernel,
        name="send",
        out_shape=(
            pltpu.VMEM((rows, 3 * span + span // 2), BF16),
            pltpu.VMEM((seqs, span), BF16),
        ),
        in_specs=[IN_VMEM] * 4 + [ANY] * len(swapped),
        out_specs=(IN_VMEM, IN_VMEM),
        compiler_params=pltpu.CompilerParams(vmem_limit_bytes=8 * MIB),
    )(at_vmem(crossed), tok, gain, at_vmem(taken), *swapped)


def experts_kernel(n_tp, arrived, shared, *refs):
    own, swapped, shards_of, refs = refs[:3], refs[3:6], refs[6:10], refs[10:]
    out_ref, down, spread, held, sems = refs[0], refs[1], refs[2], refs[3:6], refs[6]
    width = shared.shape[0] * shared.shape[1]
    copies = [pltpu.make_async_copy(own[i], held[i], sems.at[i]) for i in range(3)]
    for copy in copies:
        copy.start()
    rows, span = arrived.shape[0], out_ref.shape[2]
    each = 2 * n_tp
    chips = rows // each
    for j in range(spread.shape[0]):
        spread[j] = arrived[:, j * LANES : (j + 1) * LANES].astype(F32)

    def gathered(k, column):
        return jnp.concatenate(
            [
                spread[column // LANES + j, pl.ds(k * n_tp + q, chips, stride=each), :]
                for q in range(n_tp)
                for j in range(span // LANES)
            ],
            axis=1,
        )

    last = [spread[3 * span // LANES, pl.ds(i, chips, stride=each), :] for i in range(each)]
    tokens = [gathered(0, 2 * span), gathered(1, 2 * span), jnp.concatenate(last, axis=1)]
    tokens = jnp.concatenate(tokens, axis=0).astype(BF16)
    gate_row = shared[...].astype(F32)
    gate_row = jnp.concatenate([gate_row[i : i + 1] for i in range(gate_row.shape[0])], axis=1)
    gate_rows = jnp.broadcast_to(gate_row, (8, gate_row.shape[1])).astype(BF16)
    mix_gate = dot_nt(tokens, gate_rows)[:, :1]
    mix_gate = 1.0 / (1.0 + jnp.exp(-mix_gate))
    gate = dot_nt(tokens, jnp.concatenate([w[:, :width] for w in shards_of], axis=0))
    up = dot_nt(tokens, jnp.concatenate([w[:, width : 2 * width] for w in shards_of], axis=0))
    down[...] = jnp.concatenate([w[:, 2 * width :] for w in shards_of], axis=0)
    hidden = (mix_gate * (gate / (1.0 + jnp.exp(-gate)) * up)).astype(BF16)
    taken = chips * 2 * CAP
    for t in range(n_tp):
        out_ref[t, taken:, :] = hidden
    for o in (1, 0):
        tokens = [gathered(k, o * span) for k in range(CAP)]
        tokens = jnp.concatenate(tokens, axis=0).astype(BF16)
        gate_w, up_w, down_w = (held, swapped)[o]
        if o == 0:
            copies[0].wait()
        gate = dot(tokens, gate_w[...])
        if o == 0:
            copies[1].wait()
        up = dot(tokens, up_w[...])
        hidden = (gate / (1.0 + jnp.exp(-gate)) * up).astype(BF16)
        if o == 0:
            copies[2].wait()
        part = dot(hidden, down_w[...]).astype(BF16)
        for t in range(n_tp):
            out_ref[t, o * chips * CAP : (o + 1) * chips * CAP, :] = part[:, t * span : (t + 1) * span]


def experts(n_tp, span, arrived, shared, own, swapped, shards_of):
    rows = arrived.shape[0]
    chips = rows // (2 * n_tp)
    units = sum(w.shape[0] for w in shards_of)
    return pl.pallas_call(
        functools.partial(experts_kernel, n_tp),
        name="experts",
        out_shape=(
            pltpu.VMEM((n_tp, chips * 2 * CAP + chips * 3, span), BF16),
            pltpu.VMEM((units, span), BF16),
        ),
        in_specs=[IN_VMEM] * 2 + [ANY] * 3 + [IN_VMEM] * 7,
        out_specs=(IN_VMEM, IN_VMEM),
        scratch_shapes=[pltpu.VMEM((arrived.shape[1] // LANES, rows, LANES), F32)]
        + [pltpu.VMEM(w.shape, w.dtype) for w in own]
        + [pltpu.SemaphoreType.DMA((3,))],
        compiler_params=pltpu.CompilerParams(vmem_limit_bytes=16 * MIB),
    )(at_vmem(arrived), shared, *[at_hbm(w) for w in own], *[at_vmem(w) for w in (*swapped, *shards_of)])


def combine_kernel(crossed, down, out_ref, spread):
    n_tp, _, span = crossed.shape
    chips, each, _ = out_ref.shape
    block = chips * CAP
    taken = 2 * block
    total = crossed[0, :taken].astype(F32)
    for t in range(1, n_tp):
        total = total + crossed[t, :taken].astype(F32)
    parts = []
    for t in range(n_tp):
        part = dot(crossed[t, taken:], down[...])
        parts += [part[k * chips : (k + 1) * chips] for k in range(part.shape[0] // chips)]
    parts += [total[i * chips : (i + 1) * chips] for i in range(2 * CAP)]
    for i, part in enumerate(parts):
        for j in range(span // LANES):
            spread[i // each * (span // LANES) + j, pl.ds(i % each, chips, stride=each), :] = part[
                :, j * LANES : (j + 1) * LANES
            ]
    for j in range(spread.shape[0]):
        column = spread[j].astype(BF16).reshape(chips, each, LANES)
        out_ref[:, :, j * LANES : (j + 1) * LANES] = column


def combine(crossed, down, chips):
    n_tp, _, span = crossed.shape
    each = 2 * n_tp
    return pl.pallas_call(
        combine_kernel,
        name="combine",
        out_shape=pltpu.VMEM((chips, each, 2 * span), BF16),
        in_specs=[IN_VMEM] * 2,
        out_specs=IN_VMEM,
        scratch_shapes=[pltpu.VMEM((2 * span // LANES, chips * each, LANES), F32)],
        compiler_params=pltpu.CompilerParams(vmem_limit_bytes=8 * MIB),
    )(at_vmem(crossed), at_vmem(down))


def finish_kernel(arrived, place, residual, out_ref):
    span = residual.shape[1]
    left, right = arrived[:, :span], arrived[:, span:]
    total = dot(place[0], left) + (dot(place[1], right) + dot(place[2], right))
    out_ref[...] = (residual[...].astype(F32) + total).astype(BF16)


def finish(arrived, place, residual):
    return pl.pallas_call(
        finish_kernel,
        name="finish",
        out_shape=jax.ShapeDtypeStruct(residual.shape, BF16),
        in_specs=[IN_VMEM] * 3,
        out_specs=IN_VMEM,
        compiler_params=pltpu.CompilerParams(vmem_limit_bytes=8 * MIB),
    )(at_vmem(arrived), at_vmem(place), at_vmem(residual))


def shards(
    tokens,
    attn_gain,
    w_query,
    w_key,
    w_value,
    w_forget,
    forget_bias,
    query_gain,
    key_gain,
    cache_pairs,
    cache_cum,
    lengths,
    w_output,
    ffn_gain,
    expert_ids,
    route_weight,
    w_exp_gate,
    w_exp_up,
    w_exp_down,
    shared_gate,
    w_dense_gate,
    w_dense_up,
    w_dense_down,
):
    seqs, width = tokens.shape
    n_tp, chips = lax.axis_size("tp"), lax.axis_size(FAR)
    span = width // n_tp

    def other(w):
        return lax.ppermute(w, "ep_2", [(0, 1), (1, 0)])

    def neighbour(w, flip):
        axes = ("ep_1", "ep_2")
        return lax.ppermute(w, axes, [(i, i ^ flip) for i in range(lax.axis_size(axes))])

    own = [w_exp_gate[0], w_exp_up[0], w_exp_down[0]]
    swapped = [other(w) for w in own]
    taken, place, packed = prepare(
        n_tp, chips, seqs, expert_ids.T, route_weight.T, (w_dense_gate, w_dense_up, w_dense_down)
    )
    near, far, across = neighbour(packed, 2), neighbour(packed, 3), neighbour(packed, 1)
    partial = attend(
        n_tp,
        lengths,
        forget_bias,
        packed,
        tokens,
        attn_gain[None],
        w_query,
        w_key.T,
        w_value.T,
        w_forget.T,
        query_gain[None],
        key_gain[None],
        cache_cum,
        w_output,
        cache_pairs[:, 0],
    )
    crossed = lax.all_to_all(partial, "tp", 0, 0, tiled=True)
    message, own_residual = send(crossed, tokens, ffn_gain[None], taken, chips, [*swapped, near, across, far])
    arrived = lax.all_to_all(message.reshape(chips, -1, message.shape[1]), FAR, 0, 0, tiled=True)
    blocks, down = experts(
        n_tp,
        span,
        arrived.reshape(message.shape),
        shared_gate.reshape(-1, LANES),
        own,
        swapped,
        (packed, near, across, far),
    )
    crossed = lax.all_to_all(blocks, "tp", 0, 0, tiled=True)
    total = combine(crossed, down, chips)
    arrived = lax.all_to_all(total, FAR, 0, 0, tiled=True)
    return finish(arrived.reshape(-1, arrived.shape[2]), place, own_residual)


def solution(mesh):
    split = Mesh(mesh.devices.reshape(8, 4, 2, mesh.shape["tp"]), ("ep_0", "ep_1", "ep_2", "tp"))
    return jax.shard_map(
        shards,
        mesh=split,
        in_specs=(
            P(EP, None),
            P(),
            P(None, "tp"),
            P(None, "tp"),
            P(None, "tp"),
            P(None, "tp"),
            P("tp"),
            P(),
            P(),
            P(EP, "tp", None, None),
            P(EP, "tp", None),
            P(EP),
            P("tp", None),
            P(),
            P(),
            P(),
            P(EP, None, "tp"),
            P(EP, None, "tp"),
            P(EP, "tp", None),
            P(),
            P(EP, None),
            P(EP, None),
            P(EP, "tp"),
        ),
        out_specs=P(EP, "tp"),
        check_vma=False,
    )
```

```python
import functools

import jax
import jax.numpy as jnp
from jax import lax
from jax.experimental import pallas as pl
from jax.experimental.pallas import tpu as pltpu
from jax.sharding import Mesh
from jax.sharding import PartitionSpec as P


EP = ("ep_0", "ep_1", "ep_2")
FAR = ("ep_0", "ep_1")
EPSILON = 1e-06
F32, BF16 = jnp.float32, jnp.bfloat16
CAP = 2
LANES = 128
MIB = 1 << 20
ANY = pl.BlockSpec(memory_space=pl.ANY)
IN_VMEM = pl.BlockSpec(memory_space=pltpu.VMEM)
IN_SMEM = pl.BlockSpec(memory_space=pltpu.SMEM)
NT = (((1,), (1,)), ((), ()))


def at_hbm(x):
    return pltpu.with_memory_space_constraint(x, pltpu.HBM)


def at_vmem(x):
    return pltpu.with_memory_space_constraint(x, pltpu.VMEM)


def normal_rows(values, gain_row):
    mean_square = jnp.mean(values * values, axis=-1, keepdims=True)
    return values * lax.rsqrt(mean_square + EPSILON) * gain_row


def dot(a, b):
    return jnp.dot(a, b, preferred_element_type=F32)


def dot_nt(a, b):
    return lax.dot_general(a, b, NT, preferred_element_type=F32)


def rows_of(shape):
    return lax.broadcasted_iota(jnp.int32, shape, 0)


def lanes_of(shape):
    return lax.broadcasted_iota(jnp.int32, shape, 1)


def route_tables(ids, weights, taken_ref, place_ref):
    n_tp, n_core = lax.axis_size("tp"), lax.axis_size("ep_2")
    core_at, chip_at = lax.axis_index("ep_2"), lax.axis_index(FAR)
    rows, wide = taken_ref.shape[1:]
    batch = ids.shape[1]
    seqs = wide // n_tp
    each = 2 * n_tp
    cores = (core_at, 1 - core_at)
    base = (chip_at * n_core + core_at) * seqs
    ids, weights = ids[...].astype(F32), weights[...]

    own = lanes_of((wide, batch)) == base + rows_of((wide, batch)) % seqs
    padded = jnp.concatenate([ids, jnp.zeros((6, batch), F32)], axis=0).astype(BF16)
    own_ids = dot_nt(padded, jnp.where(own, 1.0, 0.0).astype(BF16)).astype(jnp.int32)
    row, lane = rows_of((rows, wide)), lanes_of((rows, wide))
    piece_fits = lane // seqs == row % n_tp
    slot = (row % each) // n_tp
    first, second = rows_of((wide, wide)), lanes_of((wide, wide))
    ahead = (first // seqs == second // seqs) & (first <= second)
    ahead = jnp.where(ahead, 1.0, 0.0).astype(BF16)
    for o in range(2):
        expert = (row // each) * n_core + cores[o]
        hit = (expert == own_ids[0:1, :]) | (expert == own_ids[1:2, :])
        rank = dot(jnp.where(hit, 1.0, 0.0).astype(BF16), ahead).astype(jnp.int32)
        taken = hit & (rank == slot + 1) & piece_fits
        taken_ref[o] = jnp.where(taken, 1.0, 0.0).astype(BF16)

    mine = lanes_of((seqs, batch)) == base + rows_of((seqs, batch))

    def column(values):
        return jnp.sum(jnp.where(mine, values, 0.0), axis=1, keepdims=True)

    lane = lanes_of((seqs, rows))
    slot = lane % each - 2 * CAP
    expert = (lane // each) * n_core + jnp.where(slot < CAP, cores[0], cores[1])
    weight = jnp.zeros((seqs, rows), F32)
    hit = jnp.zeros((seqs, rows), F32)
    for i in range(ids.shape[0]):
        fits = column(ids[i : i + 1]).astype(jnp.int32) == expert
        weight = jnp.where(fits, column(weights[i : i + 1]), weight)
        hit = jnp.where(fits, 1.0, hit)
    before = rows_of((seqs, seqs)) >= lanes_of((seqs, seqs))
    rank = dot(jnp.where(before, 1.0, 0.0).astype(BF16), hit.astype(BF16)).astype(jnp.int32)
    put = (slot >= 0) & (hit > 0.5) & (rank == slot % CAP + 1)
    weight = jnp.where(put, weight, 0.0)
    high = weight.astype(BF16).astype(F32)

    token, place_at = rows_of((seqs, rows)), lane % each
    share = seqs // n_tp
    part = share // 2

    def fits(index):
        return token == (index // part) * share + ((lane // each) % 2) * part + index % part

    first = jnp.where(fits(place_at), 1.0, 0.0)
    second = jnp.where((place_at < 2 * CAP) & fits(place_at + each), 1.0, 0.0)
    for i, table in enumerate((first, second + high, weight - high)):
        place_ref[i] = table.astype(BF16)


def prepare_kernel(ids_hbm, weights_hbm, *refs):
    dense, (taken_ref, place_ref, packed, ids, weights, sems) = refs[:3], refs[3:]
    copies = [
        pltpu.make_async_copy(ids_hbm, ids, sems.at[0]),
        pltpu.make_async_copy(weights_hbm, weights, sems.at[1]),
    ]
    at = 0
    for i, source in enumerate(dense):
        into = packed.at[:, at : at + source.shape[1]]
        copies.append(pltpu.make_async_copy(source, into, sems.at[2 + i]))
        at += source.shape[1]
    for copy in copies:
        copy.start()
    for copy in copies[:2]:
        copy.wait()
    route_tables(ids, weights, taken_ref, place_ref)
    for copy in copies[2:]:
        copy.wait()


def prepare(n_tp, chips, seqs, ids, weights, dense):
    return pl.pallas_call(
        prepare_kernel,
        name="prepare",
        out_shape=(
            pltpu.VMEM((2, chips * 2 * n_tp, n_tp * seqs), BF16),
            pltpu.VMEM((3, seqs, chips * 2 * n_tp), BF16),
            pltpu.VMEM((dense[0].shape[0], sum(w.shape[1] for w in dense)), BF16),
        ),
        in_specs=[ANY] * 5,
        out_specs=(IN_VMEM,) * 3,
        scratch_shapes=[
            pltpu.VMEM(ids.shape, ids.dtype),
            pltpu.VMEM(weights.shape, weights.dtype),
            pltpu.SemaphoreType.DMA((5,)),
        ],
        compiler_params=pltpu.CompilerParams(vmem_limit_bytes=8 * MIB),
    )(at_hbm(ids), at_hbm(weights), *[at_hbm(w) for w in dense])


def attend_kernel(chunks, forget_bias, lens_hbm, after, *refs):
    ahead, refs = refs[:3], refs[3:]
    sources, out_ref, fetched, rest = refs[:11], refs[11], refs[12:15], refs[15:]
    held, (lens, queries, keys, values, shift, scores, mixed, sems) = rest[:11], rest[11:]
    tok, gain, wq, wk, wv, wf, qg, kg, cum, wo, cache = held
    seqs, slots, pair = cache.shape
    head = qg.shape[1]
    group = wq.shape[1] // head
    copies = [pltpu.make_async_copy(sources[i], held[i], sems.at[i]) for i in range(10)]
    step = seqs // chunks
    parts = [
        pltpu.make_async_copy(
            sources[10].at[pl.ds(i * step, step)], cache.at[pl.ds(i * step, step)], sems.at[10 + i]
        )
        for i in range(chunks)
    ]
    lens_copy = pltpu.make_async_copy(lens_hbm, lens, sems.at[10 + chunks])
    fetches = [pltpu.make_async_copy(ahead[i], fetched[i], sems.at[11 + chunks + i]) for i in range(3)]
    lens_copy.start()
    for copy in copies[:9]:
        copy.start()
    for part in parts:
        part.start()
    copies[9].start()
    for copy in copies[:8]:
        copy.wait()

    normed = normal_rows(tok[...].astype(F32), gain[...]).astype(BF16)
    query_raw = dot(normed, wq[...])
    key_new = normal_rows(dot_nt(normed, wk[...]), kg[...]).astype(BF16).astype(F32)
    value_new = dot_nt(normed, wv[...]).astype(BF16).astype(F32)
    blank = jnp.zeros((seqs, pair - head), F32)
    key_new = jnp.concatenate([key_new, blank], axis=1)
    value_new = jnp.concatenate([blank, value_new], axis=1)
    for h in range(group):
        query = normal_rows(query_raw[:, h * head : (h + 1) * head], qg[...])
        query = jnp.concatenate([query.astype(BF16).astype(F32), blank], axis=1)
        queries[pl.ds(h, seqs, stride=group), :] = query
        keys[pl.ds(h, seqs, stride=group), :] = key_new
        values[pl.ds(h, seqs, stride=group), :] = value_new
    forget = jnp.sum(normed.astype(F32) * wf[...].astype(F32), axis=1, keepdims=True) + forget_bias[0]
    log_gate = jnp.minimum(forget, 0.0) - jnp.log1p(jnp.exp(-jnp.abs(forget)))

    lens_copy.wait()
    row = rows_of((seqs, 1))
    length = jnp.zeros((seqs, 1), jnp.int32)
    for s in range(seqs):
        length = jnp.where(row == s, lens[s], length)
    copies[8].wait()
    position = lanes_of((seqs, slots))
    summed = cum[...].reshape(seqs, slots)
    last = jnp.sum(jnp.where(position == length - 1, summed, 0.0), axis=1, keepdims=True)
    shift[...] = jnp.where(position < length, (last + log_gate) - summed, -jnp.inf)

    multiplier = head ** (-0.5)
    own_score = jnp.sum(queries[...] * keys[...], axis=1, keepdims=True) * multiplier
    tall = 2 * group
    upper = rows_of((tall, 1)) < group
    for p in range(seqs // 2):
        if (2 * p) % step == 0:
            parts[2 * p // step].wait()
            if 2 * p // step == 0:
                for fetch in fetches:
                    fetch.start()
        query = queries[tall * p : tall * (p + 1), :].astype(BF16)
        score = jnp.where(upper, dot_nt(query, cache[2 * p]), dot_nt(query, cache[2 * p + 1]))
        moved = jnp.where(upper, shift[2 * p : 2 * p + 1, :], shift[2 * p + 1 : 2 * p + 2, :])
        scores[tall * p : tall * (p + 1), :] = score * multiplier + moved
    score = scores[...]
    peak = jnp.maximum(jnp.max(score, axis=1, keepdims=True), own_score)
    past = jnp.exp(score - peak)
    own = jnp.exp(own_score - peak)
    whole = 1.0 / (jnp.sum(past, axis=1, keepdims=True) + own)
    scores[...] = past * whole
    own_prob = (own * whole).astype(BF16).astype(F32)
    for p in range(seqs // 2):
        prob = scores[tall * p : tall * (p + 1), :].astype(BF16)
        mixed[tall * p : tall * (p + 1), :] = jnp.where(
            upper, dot(prob, cache[2 * p]), dot(prob, cache[2 * p + 1])
        )
    mixed[...] = mixed[...] + own_prob * values[...]
    copies[9].wait()
    total = jnp.zeros((seqs, wo.shape[1]), F32)
    for h in range(group):
        mix = mixed[pl.ds(h, seqs, stride=group), :][:, pair - head :].astype(BF16)
        total = total + dot(mix, wo[h * head : (h + 1) * head, :])
    partial = total.astype(BF16)
    for t in range(out_ref.shape[0]):
        out_ref[t] = partial
    for fetch in fetches:
        fetch.wait()


def attend(n_tp, lens, forget_bias, after, ahead, *arrays):
    chunks = 3
    tok, wq, qg, cache = arrays[0], arrays[2], arrays[6], arrays[10]
    seqs, slots, pair = cache.shape
    heads = wq.shape[1] // qg.shape[1]
    rows = seqs * heads
    scratch = [pltpu.VMEM(a.shape, a.dtype) for a in arrays]
    scratch += [pltpu.SMEM(lens.shape, lens.dtype)]
    scratch += [pltpu.VMEM((rows, pair), F32)] * 3
    scratch += [pltpu.VMEM((seqs, slots), F32), pltpu.VMEM((rows, slots), F32), pltpu.VMEM((rows, pair), F32)]
    scratch += [pltpu.SemaphoreType.DMA((14 + chunks,))]
    return pl.pallas_call(
        functools.partial(attend_kernel, chunks),
        name="attend",
        out_shape=(pltpu.VMEM((n_tp, *tok.shape), BF16), *(pltpu.VMEM(w.shape, BF16) for w in ahead)),
        in_specs=[IN_SMEM] + [ANY] * 16,
        out_specs=(IN_VMEM,) * 4,
        scratch_shapes=scratch,
        compiler_params=pltpu.CompilerParams(vmem_limit_bytes=16 * MIB),
    )(forget_bias, at_hbm(lens), after, *[at_hbm(a) for a in (*ahead, *arrays)])


def send_kernel(crossed, tok, gain, taken_ref, *refs):
    message, own_residual = refs[-2:]
    n_tp = crossed.shape[0]
    seqs, width = tok.shape
    rows = message.shape[0]
    span = width // n_tp
    share = seqs // n_tp
    tp_at = lax.axis_index("tp")
    attn_out = crossed[0].astype(F32)
    for t in range(1, n_tp):
        attn_out = attn_out + crossed[t].astype(F32)
    residual = (tok[...].astype(F32) + attn_out).astype(BF16)
    residual_f = residual.astype(F32)
    kept = residual[:, :span]
    for t in range(1, n_tp):
        kept = jnp.where(tp_at == t, residual[:, t * span : (t + 1) * span], kept)
    own_residual[...] = kept
    normed = normal_rows(residual_f, gain[...])
    pieces = jnp.concatenate([normed[:, q * span : (q + 1) * span] for q in range(n_tp)], axis=0)
    pieces = pieces.astype(BF16)
    wide = n_tp * seqs
    for o in range(2):
        message[:, o * span : (o + 1) * span] = dot(taken_ref[o], pieces).astype(BF16)
    each = 2 * n_tp
    both = 2 * each
    part = share // 2
    narrow = span // 2
    row, lane = rows_of((both, wide)), lanes_of((both, wide))
    token = tp_at * share + (row // each) * part + (row % each) // n_tp
    fits = (lane // seqs == row % n_tp) & (lane % seqs == token)
    block = dot(jnp.where(fits, 1.0, 0.0).astype(BF16), pieces).astype(BF16)
    block = jnp.broadcast_to(block[None], (rows // both, both, span)).reshape(rows, span)
    message[:, 2 * span : 3 * span] = block
    pieces = jnp.concatenate([normed[:, q * narrow : (q + 1) * narrow] for q in range(each)], axis=0)
    row, lane = rows_of((both, each * seqs)), lanes_of((both, each * seqs))
    token = tp_at * share + (row // each) * part + part - 1
    fits = (lane // seqs == row % each) & (lane % seqs == token)
    block = dot(jnp.where(fits, 1.0, 0.0).astype(BF16), pieces.astype(BF16)).astype(BF16)
    block = jnp.broadcast_to(block[None], (rows // both, both, narrow)).reshape(rows, narrow)
    message[:, 3 * span :] = block


def send(crossed, tok, gain, taken, chips, swapped):
    n_tp, seqs, width = crossed.shape
    span = width // n_tp
    rows = chips * 2 * n_tp
    return pl.pallas_call(
        send_kernel,
        name="send",
        out_shape=(
            pltpu.VMEM((rows, 3 * span + span // 2), BF16),
            pltpu.VMEM((seqs, span), BF16),
        ),
        in_specs=[IN_VMEM] * 4 + [ANY] * len(swapped),
        out_specs=(IN_VMEM, IN_VMEM),
        compiler_params=pltpu.CompilerParams(vmem_limit_bytes=8 * MIB),
    )(at_vmem(crossed), tok, gain, at_vmem(taken), *swapped)


def experts_kernel(n_tp, arrived, shared, *refs):
    own, swapped, shards_of, refs = refs[:3], refs[3:6], refs[6:10], refs[10:]
    out_ref, down, spread = refs
    width = shared.shape[0] * shared.shape[1]
    rows, span = arrived.shape[0], out_ref.shape[2]
    each = 2 * n_tp
    chips = rows // each
    for j in range(spread.shape[0]):
        spread[j] = arrived[:, j * LANES : (j + 1) * LANES].astype(F32)

    def gathered(k, column):
        return jnp.concatenate(
            [
                spread[column // LANES + j, pl.ds(k * n_tp + q, chips, stride=each), :]
                for q in range(n_tp)
                for j in range(span // LANES)
            ],
            axis=1,
        )

    last = [spread[3 * span // LANES, pl.ds(i, chips, stride=each), :] for i in range(each)]
    tokens = [gathered(0, 2 * span), gathered(1, 2 * span), jnp.concatenate(last, axis=1)]
    tokens = jnp.concatenate(tokens, axis=0).astype(BF16)
    gate_row = shared[...].astype(F32)
    gate_row = jnp.concatenate([gate_row[i : i + 1] for i in range(gate_row.shape[0])], axis=1)
    gate_rows = jnp.broadcast_to(gate_row, (8, gate_row.shape[1])).astype(BF16)
    mix_gate = dot_nt(tokens, gate_rows)[:, :1]
    mix_gate = 1.0 / (1.0 + jnp.exp(-mix_gate))
    gate = dot_nt(tokens, jnp.concatenate([w[:, :width] for w in shards_of], axis=0))
    up = dot_nt(tokens, jnp.concatenate([w[:, width : 2 * width] for w in shards_of], axis=0))
    down[...] = jnp.concatenate([w[:, 2 * width :] for w in shards_of], axis=0)
    hidden = (mix_gate * (gate / (1.0 + jnp.exp(-gate)) * up)).astype(BF16)
    taken = chips * 2 * CAP
    for t in range(n_tp):
        out_ref[t, taken:, :] = hidden
    for o in range(2):
        tokens = [gathered(k, o * span) for k in range(CAP)]
        tokens = jnp.concatenate(tokens, axis=0).astype(BF16)
        gate_w, up_w, down_w = (own, swapped)[o]
        gate = dot(tokens, gate_w[...])
        up = dot(tokens, up_w[...])
        hidden = (gate / (1.0 + jnp.exp(-gate)) * up).astype(BF16)
        part = dot(hidden, down_w[...]).astype(BF16)
        for t in range(n_tp):
            out_ref[t, o * chips * CAP : (o + 1) * chips * CAP, :] = part[:, t * span : (t + 1) * span]


def experts(n_tp, span, arrived, shared, own, swapped, shards_of):
    rows = arrived.shape[0]
    chips = rows // (2 * n_tp)
    units = sum(w.shape[0] for w in shards_of)
    return pl.pallas_call(
        functools.partial(experts_kernel, n_tp),
        name="experts",
        out_shape=(
            pltpu.VMEM((n_tp, chips * 2 * CAP + chips * 3, span), BF16),
            pltpu.VMEM((units, span), BF16),
        ),
        in_specs=[IN_VMEM] * 12,
        out_specs=(IN_VMEM, IN_VMEM),
        scratch_shapes=[pltpu.VMEM((arrived.shape[1] // LANES, rows, LANES), F32)],
        compiler_params=pltpu.CompilerParams(vmem_limit_bytes=8 * MIB),
    )(at_vmem(arrived), shared, *[at_vmem(w) for w in (*own, *swapped, *shards_of)])


def combine_kernel(crossed, down, out_ref, spread):
    n_tp, _, span = crossed.shape
    chips, each, _ = out_ref.shape
    block = chips * CAP
    taken = 2 * block
    total = crossed[0, :taken].astype(F32)
    for t in range(1, n_tp):
        total = total + crossed[t, :taken].astype(F32)
    parts = []
    for t in range(n_tp):
        part = dot(crossed[t, taken:], down[...])
        parts += [part[k * chips : (k + 1) * chips] for k in range(part.shape[0] // chips)]
    parts += [total[i * chips : (i + 1) * chips] for i in range(2 * CAP)]
    for i, part in enumerate(parts):
        for j in range(span // LANES):
            spread[i // each * (span // LANES) + j, pl.ds(i % each, chips, stride=each), :] = part[
                :, j * LANES : (j + 1) * LANES
            ]
    for j in range(spread.shape[0]):
        column = spread[j].astype(BF16).reshape(chips, each, LANES)
        out_ref[:, :, j * LANES : (j + 1) * LANES] = column


def combine(crossed, down, chips):
    n_tp, _, span = crossed.shape
    each = 2 * n_tp
    return pl.pallas_call(
        combine_kernel,
        name="combine",
        out_shape=pltpu.VMEM((chips, each, 2 * span), BF16),
        in_specs=[IN_VMEM] * 2,
        out_specs=IN_VMEM,
        scratch_shapes=[pltpu.VMEM((2 * span // LANES, chips * each, LANES), F32)],
        compiler_params=pltpu.CompilerParams(vmem_limit_bytes=8 * MIB),
    )(at_vmem(crossed), at_vmem(down))


def finish_kernel(arrived, place, residual, out_ref):
    span = residual.shape[1]
    left, right = arrived[:, :span], arrived[:, span:]
    total = dot(place[0], left) + (dot(place[1], right) + dot(place[2], right))
    out_ref[...] = (residual[...].astype(F32) + total).astype(BF16)


def finish(arrived, place, residual):
    return pl.pallas_call(
        finish_kernel,
        name="finish",
        out_shape=jax.ShapeDtypeStruct(residual.shape, BF16),
        in_specs=[IN_VMEM] * 3,
        out_specs=IN_VMEM,
        compiler_params=pltpu.CompilerParams(vmem_limit_bytes=8 * MIB),
    )(at_vmem(arrived), at_vmem(place), at_vmem(residual))


def shards(
    tokens,
    attn_gain,
    w_query,
    w_key,
    w_value,
    w_forget,
    forget_bias,
    query_gain,
    key_gain,
    cache_pairs,
    cache_cum,
    lengths,
    w_output,
    ffn_gain,
    expert_ids,
    route_weight,
    w_exp_gate,
    w_exp_up,
    w_exp_down,
    shared_gate,
    w_dense_gate,
    w_dense_up,
    w_dense_down,
):
    seqs, width = tokens.shape
    n_tp, chips = lax.axis_size("tp"), lax.axis_size(FAR)
    span = width // n_tp

    def other(w):
        return lax.ppermute(w, "ep_2", [(0, 1), (1, 0)])

    def neighbour(w, flip):
        axes = ("ep_1", "ep_2")
        return lax.ppermute(w, axes, [(i, i ^ flip) for i in range(lax.axis_size(axes))])

    own = [w_exp_gate[0], w_exp_up[0], w_exp_down[0]]
    swapped = [other(w) for w in own]
    taken, place, packed = prepare(
        n_tp, chips, seqs, expert_ids.T, route_weight.T, (w_dense_gate, w_dense_up, w_dense_down)
    )
    near, far, across = neighbour(packed, 2), neighbour(packed, 3), neighbour(packed, 1)
    partial, *fetched = attend(
        n_tp,
        lengths,
        forget_bias,
        packed,
        own,
        tokens,
        attn_gain[None],
        w_query,
        w_key.T,
        w_value.T,
        w_forget.T,
        query_gain[None],
        key_gain[None],
        cache_cum,
        w_output,
        cache_pairs[:, 0],
    )
    crossed = lax.all_to_all(partial, "tp", 0, 0, tiled=True)
    message, own_residual = send(crossed, tokens, ffn_gain[None], taken, chips, [*swapped, near, across, far])
    arrived = lax.all_to_all(message.reshape(chips, -1, message.shape[1]), FAR, 0, 0, tiled=True)
    blocks, down = experts(
        n_tp,
        span,
        arrived.reshape(message.shape),
        shared_gate.reshape(-1, LANES),
        fetched,
        swapped,
        (packed, near, across, far),
    )
    crossed = lax.all_to_all(blocks, "tp", 0, 0, tiled=True)
    total = combine(crossed, down, chips)
    arrived = lax.all_to_all(total, FAR, 0, 0, tiled=True)
    return finish(arrived.reshape(-1, arrived.shape[2]), place, own_residual)


def solution(mesh):
    split = Mesh(mesh.devices.reshape(8, 4, 2, mesh.shape["tp"]), ("ep_0", "ep_1", "ep_2", "tp"))
    return jax.shard_map(
        shards,
        mesh=split,
        in_specs=(
            P(EP, None),
            P(),
            P(None, "tp"),
            P(None, "tp"),
            P(None, "tp"),
            P(None, "tp"),
            P("tp"),
            P(),
            P(),
            P(EP, "tp", None, None),
            P(EP, "tp", None),
            P(EP),
            P("tp", None),
            P(),
            P(),
            P(),
            P(EP, None, "tp"),
            P(EP, None, "tp"),
            P(EP, "tp", None),
            P(),
            P(EP, None),
            P(EP, None),
            P(EP, "tp"),
        ),
        out_specs=P(EP, "tp"),
        check_vma=False,
    )
```

```python
import functools

import jax
import jax.numpy as jnp
from jax import lax
from jax.experimental import pallas as pl
from jax.experimental.pallas import tpu as pltpu
from jax.sharding import Mesh
from jax.sharding import PartitionSpec as P


EP = ("ep_0", "ep_1", "ep_2")
FAR = ("ep_0", "ep_1")
EPSILON = 1e-06
F32, BF16 = jnp.float32, jnp.bfloat16
CAP = 2
LANES = 128
MIB = 1 << 20
HEADS_ORDER = (1, 3, 2)
EXPERT_ORDER = (2, 1, 3)
ANY = pl.BlockSpec(memory_space=pl.ANY)
IN_VMEM = pl.BlockSpec(memory_space=pltpu.VMEM)
IN_SMEM = pl.BlockSpec(memory_space=pltpu.SMEM)
NT = (((1,), (1,)), ((), ()))


def at_hbm(x):
    return pltpu.with_memory_space_constraint(x, pltpu.HBM)


def at_vmem(x):
    return pltpu.with_memory_space_constraint(x, pltpu.VMEM)


def normal_rows(values, gain_row):
    mean_square = jnp.mean(values * values, axis=-1, keepdims=True)
    return values * lax.rsqrt(mean_square + EPSILON) * gain_row


def dot(a, b):
    return jnp.dot(a, b, preferred_element_type=F32)


def dot_nt(a, b):
    return lax.dot_general(a, b, NT, preferred_element_type=F32)


def rows_of(shape):
    return lax.broadcasted_iota(jnp.int32, shape, 0)


def lanes_of(shape):
    return lax.broadcasted_iota(jnp.int32, shape, 1)


def route_tables(ids, weights, taken_ref, place_ref):
    n_tp, n_core = lax.axis_size("tp"), lax.axis_size("ep_2")
    core_at, chip_at, tp_at = lax.axis_index("ep_2"), lax.axis_index(FAR), lax.axis_index("tp")
    rows, wide = taken_ref.shape[1:]
    batch = ids.shape[1]
    seqs = wide // n_tp
    each = 2 * n_tp
    cores = (core_at, 1 - core_at)
    base = (chip_at * n_core + core_at) * seqs
    ids, weights = ids[...].astype(F32), weights[...]

    own = lanes_of((wide, batch)) == base + rows_of((wide, batch)) % seqs
    padded = jnp.concatenate([ids, jnp.zeros((6, batch), F32)], axis=0).astype(BF16)
    own_ids = dot_nt(padded, jnp.where(own, 1.0, 0.0).astype(BF16)).astype(jnp.int32)
    row, lane = rows_of((rows, wide)), lanes_of((rows, wide))
    piece_fits = lane // seqs == row % n_tp
    slot = (row % each) // n_tp
    first, second = rows_of((wide, wide)), lanes_of((wide, wide))
    ahead = (first // seqs == second // seqs) & (first <= second)
    ahead = jnp.where(ahead, 1.0, 0.0).astype(BF16)
    for o in range(2):
        expert = (row // each) * n_core + cores[o]
        hit = (expert == own_ids[0:1, :]) | (expert == own_ids[1:2, :])
        rank = dot(jnp.where(hit, 1.0, 0.0).astype(BF16), ahead).astype(jnp.int32)
        taken = hit & (rank == slot + 1) & piece_fits
        taken_ref[o] = jnp.where(taken, 1.0, 0.0).astype(BF16)

    mine = lanes_of((seqs, batch)) == base + rows_of((seqs, batch))

    def column(values):
        return jnp.sum(jnp.where(mine, values, 0.0), axis=1, keepdims=True)

    lane = lanes_of((seqs, rows))
    slot = lane % each - 2 * CAP
    expert = (lane // each) * n_core + jnp.where(slot < CAP, cores[0], cores[1])
    weight = jnp.zeros((seqs, rows), F32)
    hit = jnp.zeros((seqs, rows), F32)
    for i in range(ids.shape[0]):
        fits = column(ids[i : i + 1]).astype(jnp.int32) == expert
        weight = jnp.where(fits, column(weights[i : i + 1]), weight)
        hit = jnp.where(fits, 1.0, hit)
    before = rows_of((seqs, seqs)) >= lanes_of((seqs, seqs))
    rank = dot(jnp.where(before, 1.0, 0.0).astype(BF16), hit.astype(BF16)).astype(jnp.int32)
    put = (slot >= 0) & (hit > 0.5) & (rank == slot % CAP + 1)
    weight = jnp.where(put, weight, 0.0)
    high = weight.astype(BF16).astype(F32)

    token, place_at = rows_of((seqs, rows)), lane % each
    share = seqs // n_tp
    part = share // 2

    def fits(index):
        owner = (tp_at - index // part + n_tp) % n_tp
        return token == owner * share + ((lane // each) % 2) * part + index % part

    first = jnp.where(fits(place_at), 1.0, 0.0)
    second = jnp.where((place_at < 2 * CAP) & fits(place_at + each), 1.0, 0.0)
    for i, table in enumerate((first, second + high, weight - high)):
        place_ref[i] = table.astype(BF16)


def tables_kernel(ids_hbm, weights_hbm, after, taken_ref, place_ref, ids, weights, sems):
    copies = [
        pltpu.make_async_copy(ids_hbm, ids, sems.at[0]),
        pltpu.make_async_copy(weights_hbm, weights, sems.at[1]),
    ]
    for copy in copies:
        copy.start()
    for copy in copies:
        copy.wait()
    route_tables(ids, weights, taken_ref, place_ref)


def tables(n_tp, chips, seqs, ids, weights, after):
    return pl.pallas_call(
        tables_kernel,
        name="tables",
        out_shape=(
            pltpu.VMEM((2, chips * 2 * n_tp, n_tp * seqs), BF16),
            pltpu.VMEM((3, seqs, chips * 2 * n_tp), BF16),
        ),
        in_specs=[ANY] * 3,
        out_specs=(IN_VMEM,) * 2,
        scratch_shapes=[
            pltpu.VMEM(ids.shape, ids.dtype),
            pltpu.VMEM(weights.shape, weights.dtype),
            pltpu.SemaphoreType.DMA((2,)),
        ],
        compiler_params=pltpu.CompilerParams(vmem_limit_bytes=8 * MIB),
    )(at_hbm(ids), at_hbm(weights), after)


def pack_kernel(*refs):
    dense, packed, sems = refs[:3], refs[3], refs[4]
    copies, at = [], 0
    for i, source in enumerate(dense):
        into = packed.at[:, at : at + source.shape[1]]
        copies.append(pltpu.make_async_copy(source, into, sems.at[i]))
        at += source.shape[1]
    for copy in copies:
        copy.start()
    for copy in copies:
        copy.wait()


def pack(dense):
    return pl.pallas_call(
        pack_kernel,
        name="pack",
        out_shape=pltpu.VMEM((dense[0].shape[0], sum(w.shape[1] for w in dense)), BF16),
        in_specs=[ANY] * 3,
        out_specs=IN_VMEM,
        scratch_shapes=[pltpu.SemaphoreType.DMA((3,))],
        compiler_params=pltpu.CompilerParams(vmem_limit_bytes=1 * MIB),
    )(*[at_hbm(w) for w in dense])


def attend_kernel(chunks, forget_bias, lens_hbm, after, *refs):
    ahead, refs = refs[:3], refs[3:]
    sources, out_ref, fetched, rest = refs[:11], refs[11], refs[12:15], refs[15:]
    held, (lens, queries, keys, values, shift, scores, mixed, sems) = rest[:11], rest[11:]
    tok, gain, wq, wk, wv, wf, qg, kg, cum, wo, cache = held
    seqs, slots, pair = cache.shape
    head = qg.shape[1]
    group = wq.shape[1] // head
    copies = [pltpu.make_async_copy(sources[i], held[i], sems.at[i]) for i in range(10)]
    step = seqs // chunks
    parts = [
        pltpu.make_async_copy(
            sources[10].at[pl.ds(i * step, step)], cache.at[pl.ds(i * step, step)], sems.at[10 + i]
        )
        for i in range(chunks)
    ]
    lens_copy = pltpu.make_async_copy(lens_hbm, lens, sems.at[10 + chunks])
    fetches = [pltpu.make_async_copy(ahead[i], fetched[i], sems.at[11 + chunks + i]) for i in range(3)]
    lens_copy.start()
    for copy in copies[:9]:
        copy.start()
    for part in parts:
        part.start()
    copies[9].start()
    for copy in copies[:8]:
        copy.wait()

    normed = normal_rows(tok[...].astype(F32), gain[...]).astype(BF16)
    query_raw = dot(normed, wq[...])
    key_new = normal_rows(dot_nt(normed, wk[...]), kg[...]).astype(BF16).astype(F32)
    value_new = dot_nt(normed, wv[...]).astype(BF16).astype(F32)
    blank = jnp.zeros((seqs, pair - head), F32)
    key_new = jnp.concatenate([key_new, blank], axis=1)
    value_new = jnp.concatenate([blank, value_new], axis=1)
    for h in range(group):
        query = normal_rows(query_raw[:, h * head : (h + 1) * head], qg[...])
        query = jnp.concatenate([query.astype(BF16).astype(F32), blank], axis=1)
        queries[pl.ds(h, seqs, stride=group), :] = query
        keys[pl.ds(h, seqs, stride=group), :] = key_new
        values[pl.ds(h, seqs, stride=group), :] = value_new
    forget = jnp.sum(normed.astype(F32) * wf[...].astype(F32), axis=1, keepdims=True) + forget_bias[0]
    log_gate = jnp.minimum(forget, 0.0) - jnp.log1p(jnp.exp(-jnp.abs(forget)))

    lens_copy.wait()
    row = rows_of((seqs, 1))
    length = jnp.zeros((seqs, 1), jnp.int32)
    for s in range(seqs):
        length = jnp.where(row == s, lens[s], length)
    copies[8].wait()
    position = lanes_of((seqs, slots))
    summed = cum[...].reshape(seqs, slots)
    last = jnp.sum(jnp.where(position == length - 1, summed, 0.0), axis=1, keepdims=True)
    shift[...] = jnp.where(position < length, (last + log_gate) - summed, -jnp.inf)

    multiplier = head ** (-0.5)
    own_score = jnp.sum(queries[...] * keys[...], axis=1, keepdims=True) * multiplier
    tall = 2 * group
    upper = rows_of((tall, 1)) < group
    for p in range(seqs // 2):
        if (2 * p) % step == 0:
            parts[2 * p // step].wait()
            if 2 * p // step == 0:
                for fetch in fetches:
                    fetch.start()
        query = queries[tall * p : tall * (p + 1), :].astype(BF16)
        score = jnp.where(upper, dot_nt(query, cache[2 * p]), dot_nt(query, cache[2 * p + 1]))
        moved = jnp.where(upper, shift[2 * p : 2 * p + 1, :], shift[2 * p + 1 : 2 * p + 2, :])
        scores[tall * p : tall * (p + 1), :] = score * multiplier + moved
    score = scores[...]
    peak = jnp.maximum(jnp.max(score, axis=1, keepdims=True), own_score)
    past = jnp.exp(score - peak)
    own = jnp.exp(own_score - peak)
    whole = 1.0 / (jnp.sum(past, axis=1, keepdims=True) + own)
    scores[...] = past * whole
    own_prob = (own * whole).astype(BF16).astype(F32)
    for p in range(seqs // 2):
        prob = scores[tall * p : tall * (p + 1), :].astype(BF16)
        mixed[tall * p : tall * (p + 1), :] = jnp.where(
            upper, dot(prob, cache[2 * p]), dot(prob, cache[2 * p + 1])
        )
    mixed[...] = mixed[...] + own_prob * values[...]
    copies[9].wait()
    total = jnp.zeros((seqs, wo.shape[1]), F32)
    for h in range(group):
        mix = mixed[pl.ds(h, seqs, stride=group), :][:, pair - head :].astype(BF16)
        total = total + dot(mix, wo[h * head : (h + 1) * head, :])
    partial = total.astype(BF16)
    out_ref[...] = partial
    for fetch in fetches:
        fetch.wait()


def attend(lens, forget_bias, after, ahead, *arrays):
    chunks = 3
    tok, wq, qg, cache = arrays[0], arrays[2], arrays[6], arrays[10]
    seqs, slots, pair = cache.shape
    heads = wq.shape[1] // qg.shape[1]
    rows = seqs * heads
    scratch = [pltpu.VMEM(a.shape, a.dtype) for a in arrays]
    scratch += [pltpu.SMEM(lens.shape, lens.dtype)]
    scratch += [pltpu.VMEM((rows, pair), F32)] * 3
    scratch += [pltpu.VMEM((seqs, slots), F32), pltpu.VMEM((rows, slots), F32), pltpu.VMEM((rows, pair), F32)]
    scratch += [pltpu.SemaphoreType.DMA((14 + chunks,))]
    return pl.pallas_call(
        functools.partial(attend_kernel, chunks),
        name="attend",
        out_shape=(pltpu.VMEM(tok.shape, BF16), *(pltpu.VMEM(w.shape, BF16) for w in ahead)),
        in_specs=[IN_SMEM] + [ANY] * 16,
        out_specs=(IN_VMEM,) * 4,
        scratch_shapes=scratch,
        compiler_params=pltpu.CompilerParams(vmem_limit_bytes=16 * MIB),
    )(forget_bias, at_hbm(lens), after, *[at_hbm(a) for a in (*ahead, *arrays)])


def send_kernel(n_tp, *refs):
    crossed, (tok, gain, taken_ref), (message, own_residual) = refs[:n_tp], refs[n_tp : n_tp + 3], refs[-2:]
    seqs, width = tok.shape
    rows = message.shape[0]
    span = width // n_tp
    share = seqs // n_tp
    tp_at = lax.axis_index("tp")
    attn_out = crossed[0][...].astype(F32)
    for t in range(1, n_tp):
        attn_out = attn_out + crossed[t][...].astype(F32)
    residual = (tok[...].astype(F32) + attn_out).astype(BF16)
    residual_f = residual.astype(F32)
    kept = residual[:, :span]
    for t in range(1, n_tp):
        kept = jnp.where(tp_at == t, residual[:, t * span : (t + 1) * span], kept)
    own_residual[...] = kept
    normed = normal_rows(residual_f, gain[...])
    pieces = jnp.concatenate([normed[:, q * span : (q + 1) * span] for q in range(n_tp)], axis=0)
    pieces = pieces.astype(BF16)
    wide = n_tp * seqs
    for o in range(2):
        message[:, o * span : (o + 1) * span] = dot(taken_ref[o], pieces).astype(BF16)
    each = 2 * n_tp
    both = 2 * each
    part = share // 2
    narrow = span // 2
    row, lane = rows_of((both, wide)), lanes_of((both, wide))
    token = tp_at * share + (row // each) * part + (row % each) // n_tp
    fits = (lane // seqs == row % n_tp) & (lane % seqs == token)
    block = dot(jnp.where(fits, 1.0, 0.0).astype(BF16), pieces).astype(BF16)
    block = jnp.broadcast_to(block[None], (rows // both, both, span)).reshape(rows, span)
    message[:, 2 * span : 3 * span] = block
    pieces = jnp.concatenate([normed[:, q * narrow : (q + 1) * narrow] for q in range(each)], axis=0)
    row, lane = rows_of((both, each * seqs)), lanes_of((both, each * seqs))
    token = tp_at * share + (row // each) * part + part - 1
    fits = (lane // seqs == row % each) & (lane % seqs == token)
    block = dot(jnp.where(fits, 1.0, 0.0).astype(BF16), pieces.astype(BF16)).astype(BF16)
    block = jnp.broadcast_to(block[None], (rows // both, both, narrow)).reshape(rows, narrow)
    message[:, 3 * span :] = block


def send(crossed, tok, gain, taken, chips, swapped):
    n_tp = len(crossed)
    seqs, width = tok.shape
    span = width // n_tp
    rows = chips * 2 * n_tp
    return pl.pallas_call(
        functools.partial(send_kernel, n_tp),
        name="send",
        out_shape=(
            pltpu.VMEM((rows, 3 * span + span // 2), BF16),
            pltpu.VMEM((seqs, span), BF16),
        ),
        in_specs=[IN_VMEM] * (n_tp + 3) + [ANY] * len(swapped),
        out_specs=(IN_VMEM, IN_VMEM),
        compiler_params=pltpu.CompilerParams(vmem_limit_bytes=8 * MIB),
    )(*[at_vmem(part) for part in crossed], tok, gain, at_vmem(taken), *swapped)


def experts_kernel(n_tp, arrived, shared, *refs):
    own, swapped, shards_of, refs = refs[:3], refs[3:6], refs[6:10], refs[10:]
    blocks, (down, spread) = refs[:n_tp], refs[n_tp:]
    tp_at = lax.axis_index("tp")
    width = shared.shape[0] * shared.shape[1]
    rows, span = arrived.shape[0], blocks[0].shape[1]
    each = 2 * n_tp
    chips = rows // each
    for j in range(spread.shape[0]):
        spread[j] = arrived[:, j * LANES : (j + 1) * LANES].astype(F32)

    def gathered(k, column):
        return jnp.concatenate(
            [
                spread[column // LANES + j, pl.ds(k * n_tp + q, chips, stride=each), :]
                for q in range(n_tp)
                for j in range(span // LANES)
            ],
            axis=1,
        )

    last = [spread[3 * span // LANES, pl.ds(i, chips, stride=each), :] for i in range(each)]
    tokens = [gathered(0, 2 * span), gathered(1, 2 * span), jnp.concatenate(last, axis=1)]
    tokens = jnp.concatenate(tokens, axis=0).astype(BF16)
    gate_row = shared[...].astype(F32)
    gate_row = jnp.concatenate([gate_row[i : i + 1] for i in range(gate_row.shape[0])], axis=1)
    gate_rows = jnp.broadcast_to(gate_row, (8, gate_row.shape[1])).astype(BF16)
    mix_gate = dot_nt(tokens, gate_rows)[:, :1]
    mix_gate = 1.0 / (1.0 + jnp.exp(-mix_gate))
    gate = dot_nt(tokens, jnp.concatenate([w[:, :width] for w in shards_of], axis=0))
    up = dot_nt(tokens, jnp.concatenate([w[:, width : 2 * width] for w in shards_of], axis=0))
    down[...] = jnp.concatenate([w[:, 2 * width :] for w in shards_of], axis=0)
    hidden = (mix_gate * (gate / (1.0 + jnp.exp(-gate)) * up)).astype(BF16)
    taken = chips * 2 * CAP
    for block in blocks:
        block[taken:, :] = hidden
    for o in range(2):
        tokens = [gathered(k, o * span) for k in range(CAP)]
        tokens = jnp.concatenate(tokens, axis=0).astype(BF16)
        gate_w, up_w, down_w = (own, swapped)[o]
        gate = dot(tokens, gate_w[...])
        up = dot(tokens, up_w[...])
        hidden = (gate / (1.0 + jnp.exp(-gate)) * up).astype(BF16)
        part = dot(hidden, down_w[...]).astype(BF16)
        parts = [part[:, t * span : (t + 1) * span] for t in range(n_tp)]
        for k in range(n_tp):
            chosen = parts[k]
            for t in range(1, n_tp):
                chosen = jnp.where(tp_at == t, parts[(t + k) % n_tp], chosen)
            blocks[k][o * chips * CAP : (o + 1) * chips * CAP, :] = chosen


def experts(n_tp, span, arrived, shared, own, swapped, shards_of):
    rows = arrived.shape[0]
    chips = rows // (2 * n_tp)
    units = sum(w.shape[0] for w in shards_of)
    return pl.pallas_call(
        functools.partial(experts_kernel, n_tp),
        name="experts",
        out_shape=(
            *[pltpu.VMEM((chips * 2 * CAP + chips * 3, span), BF16)] * n_tp,
            pltpu.VMEM((units, span), BF16),
        ),
        in_specs=[IN_VMEM] * 12,
        out_specs=(IN_VMEM,) * (n_tp + 1),
        scratch_shapes=[pltpu.VMEM((arrived.shape[1] // LANES, rows, LANES), F32)],
        compiler_params=pltpu.CompilerParams(vmem_limit_bytes=8 * MIB),
    )(at_vmem(arrived), shared, *[at_vmem(w) for w in (*own, *swapped, *shards_of)])


def combine_kernel(n_tp, *refs):
    crossed, (down, out_ref, spread) = refs[:n_tp], refs[n_tp:]
    span = down.shape[1]
    chips, each, _ = out_ref.shape
    block = chips * CAP
    taken = 2 * block
    total = crossed[0][:taken].astype(F32)
    for t in range(1, n_tp):
        total = total + crossed[t][:taken].astype(F32)
    parts = []
    for t in range(n_tp):
        part = dot(crossed[t][taken:], down[...])
        parts += [part[k * chips : (k + 1) * chips] for k in range(part.shape[0] // chips)]
    parts += [total[i * chips : (i + 1) * chips] for i in range(2 * CAP)]
    for i, part in enumerate(parts):
        for j in range(span // LANES):
            spread[i // each * (span // LANES) + j, pl.ds(i % each, chips, stride=each), :] = part[
                :, j * LANES : (j + 1) * LANES
            ]
    for j in range(spread.shape[0]):
        column = spread[j].astype(BF16).reshape(chips, each, LANES)
        out_ref[:, :, j * LANES : (j + 1) * LANES] = column


def combine(crossed, down, chips):
    n_tp, span = len(crossed), down.shape[1]
    each = 2 * n_tp
    return pl.pallas_call(
        functools.partial(combine_kernel, n_tp),
        name="combine",
        out_shape=pltpu.VMEM((chips, each, 2 * span), BF16),
        in_specs=[IN_VMEM] * (n_tp + 1),
        out_specs=IN_VMEM,
        scratch_shapes=[pltpu.VMEM((2 * span // LANES, chips * each, LANES), F32)],
        compiler_params=pltpu.CompilerParams(vmem_limit_bytes=8 * MIB),
    )(*[at_vmem(block) for block in crossed], at_vmem(down))


def finish_kernel(arrived, place, residual, out_ref):
    span = residual.shape[1]
    left, right = arrived[:, :span], arrived[:, span:]
    total = dot(place[0], left) + (dot(place[1], right) + dot(place[2], right))
    out_ref[...] = (residual[...].astype(F32) + total).astype(BF16)


def finish(arrived, place, residual):
    return pl.pallas_call(
        finish_kernel,
        name="finish",
        out_shape=jax.ShapeDtypeStruct(residual.shape, BF16),
        in_specs=[IN_VMEM] * 3,
        out_specs=IN_VMEM,
        compiler_params=pltpu.CompilerParams(vmem_limit_bytes=8 * MIB),
    )(at_vmem(arrived), at_vmem(place), at_vmem(residual))


def shards(
    tokens,
    attn_gain,
    w_query,
    w_key,
    w_value,
    w_forget,
    forget_bias,
    query_gain,
    key_gain,
    cache_pairs,
    cache_cum,
    lengths,
    w_output,
    ffn_gain,
    expert_ids,
    route_weight,
    w_exp_gate,
    w_exp_up,
    w_exp_down,
    shared_gate,
    w_dense_gate,
    w_dense_up,
    w_dense_down,
):
    seqs, width = tokens.shape
    n_tp, chips = lax.axis_size("tp"), lax.axis_size(FAR)
    span = width // n_tp

    def other(w):
        return lax.ppermute(w, "ep_2", [(0, 1), (1, 0)])

    def neighbour(w, flip):
        axes = ("ep_1", "ep_2")
        return lax.ppermute(w, axes, [(i, i ^ flip) for i in range(lax.axis_size(axes))])

    def passed_on(x, k):
        return lax.ppermute(x, "tp", [(i, (i + k) % n_tp) for i in range(n_tp)])

    own = [w_exp_gate[0], w_exp_up[0], w_exp_down[0]]
    swapped = [other(w) for w in own]
    packed = pack((w_dense_gate, w_dense_up, w_dense_down))
    near, far, across = neighbour(packed, 2), neighbour(packed, 3), neighbour(packed, 1)
    partial, *fetched = attend(
        lengths,
        forget_bias,
        packed,
        own,
        tokens,
        attn_gain[None],
        w_query,
        w_key.T,
        w_value.T,
        w_forget.T,
        query_gain[None],
        key_gain[None],
        cache_cum,
        w_output,
        cache_pairs[:, 0],
    )
    crossed = [partial] + [passed_on(partial, k) for k in HEADS_ORDER]
    taken, place = tables(n_tp, chips, seqs, expert_ids.T, route_weight.T, partial)
    message, own_residual = send(crossed, tokens, ffn_gain[None], taken, chips, [*swapped, near, across, far])
    arrived = lax.all_to_all(message.reshape(chips, -1, message.shape[1]), FAR, 0, 0, tiled=True)
    *blocks, down = experts(
        n_tp,
        span,
        arrived.reshape(message.shape),
        shared_gate.reshape(-1, LANES),
        fetched,
        swapped,
        (packed, near, across, far),
    )
    crossed = [passed_on(blocks[k], k) for k in EXPERT_ORDER]
    crossed = [blocks[0]] + [crossed[EXPERT_ORDER.index(k)] for k in range(1, n_tp)]
    total = combine(crossed, down, chips)
    arrived = lax.all_to_all(total, FAR, 0, 0, tiled=True)
    return finish(arrived.reshape(-1, arrived.shape[2]), place, own_residual)


def solution(mesh):
    split = Mesh(mesh.devices.reshape(8, 4, 2, mesh.shape["tp"]), ("ep_0", "ep_1", "ep_2", "tp"))
    return jax.shard_map(
        shards,
        mesh=split,
        in_specs=(
            P(EP, None),
            P(),
            P(None, "tp"),
            P(None, "tp"),
            P(None, "tp"),
            P(None, "tp"),
            P("tp"),
            P(),
            P(),
            P(EP, "tp", None, None),
            P(EP, "tp", None),
            P(EP),
            P("tp", None),
            P(),
            P(),
            P(),
            P(EP, None, "tp"),
            P(EP, None, "tp"),
            P(EP, "tp", None),
            P(),
            P(EP, None),
            P(EP, None),
            P(EP, "tp"),
        ),
        out_specs=P(EP, "tp"),
        check_vma=False,
    )
```

```python
import functools

import jax
import jax.numpy as jnp
from jax import lax
from jax.experimental import pallas as pl
from jax.experimental.pallas import tpu as pltpu
from jax.sharding import Mesh
from jax.sharding import PartitionSpec as P


EP = ("ep_0", "ep_1", "ep_2")
FAR = ("ep_0", "ep_1")
EPSILON = 1e-06
F32, BF16 = jnp.float32, jnp.bfloat16
CAP = 2
LANES = 128
MIB = 1 << 20
HEADS_ORDER = (2, 1, 3)
EXPERT_ORDER = (1, 3, 2)
ANY = pl.BlockSpec(memory_space=pl.ANY)
IN_VMEM = pl.BlockSpec(memory_space=pltpu.VMEM)
IN_SMEM = pl.BlockSpec(memory_space=pltpu.SMEM)
NT = (((1,), (1,)), ((), ()))


def at_hbm(x):
    return pltpu.with_memory_space_constraint(x, pltpu.HBM)


def at_vmem(x):
    return pltpu.with_memory_space_constraint(x, pltpu.VMEM)


def normal_rows(values, gain_row):
    mean_square = jnp.mean(values * values, axis=-1, keepdims=True)
    return values * lax.rsqrt(mean_square + EPSILON) * gain_row


def dot(a, b):
    return jnp.dot(a, b, preferred_element_type=F32)


def dot_nt(a, b):
    return lax.dot_general(a, b, NT, preferred_element_type=F32)


def rows_of(shape):
    return lax.broadcasted_iota(jnp.int32, shape, 0)


def lanes_of(shape):
    return lax.broadcasted_iota(jnp.int32, shape, 1)


def route_tables(ids, weights, taken_ref, place_ref):
    n_tp, n_core = lax.axis_size("tp"), lax.axis_size("ep_2")
    core_at, chip_at, tp_at = lax.axis_index("ep_2"), lax.axis_index(FAR), lax.axis_index("tp")
    rows, wide = taken_ref.shape[1:]
    batch = ids.shape[1]
    seqs = wide // n_tp
    each = 2 * n_tp
    cores = (core_at, 1 - core_at)
    base = (chip_at * n_core + core_at) * seqs
    ids, weights = ids[...].astype(F32), weights[...]

    own = lanes_of((wide, batch)) == base + rows_of((wide, batch)) % seqs
    padded = jnp.concatenate([ids, jnp.zeros((6, batch), F32)], axis=0).astype(BF16)
    own_ids = dot_nt(padded, jnp.where(own, 1.0, 0.0).astype(BF16)).astype(jnp.int32)
    row, lane = rows_of((rows, wide)), lanes_of((rows, wide))
    piece_fits = lane // seqs == row % n_tp
    slot = (row % each) // n_tp
    first, second = rows_of((wide, wide)), lanes_of((wide, wide))
    ahead = (first // seqs == second // seqs) & (first <= second)
    ahead = jnp.where(ahead, 1.0, 0.0).astype(BF16)
    for o in range(2):
        expert = (row // each) * n_core + cores[o]
        hit = (expert == own_ids[0:1, :]) | (expert == own_ids[1:2, :])
        rank = dot(jnp.where(hit, 1.0, 0.0).astype(BF16), ahead).astype(jnp.int32)
        taken = hit & (rank == slot + 1) & piece_fits
        taken_ref[o] = jnp.where(taken, 1.0, 0.0).astype(BF16)

    mine = lanes_of((seqs, batch)) == base + rows_of((seqs, batch))

    def column(values):
        return jnp.sum(jnp.where(mine, values, 0.0), axis=1, keepdims=True)

    lane = lanes_of((seqs, rows))
    slot = lane % each - 2 * CAP
    expert = (lane // each) * n_core + jnp.where(slot < CAP, cores[0], cores[1])
    weight = jnp.zeros((seqs, rows), F32)
    hit = jnp.zeros((seqs, rows), F32)
    for i in range(ids.shape[0]):
        fits = column(ids[i : i + 1]).astype(jnp.int32) == expert
        weight = jnp.where(fits, column(weights[i : i + 1]), weight)
        hit = jnp.where(fits, 1.0, hit)
    before = rows_of((seqs, seqs)) >= lanes_of((seqs, seqs))
    rank = dot(jnp.where(before, 1.0, 0.0).astype(BF16), hit.astype(BF16)).astype(jnp.int32)
    put = (slot >= 0) & (hit > 0.5) & (rank == slot % CAP + 1)
    weight = jnp.where(put, weight, 0.0)
    high = weight.astype(BF16).astype(F32)

    token, place_at = rows_of((seqs, rows)), lane % each
    share = seqs // n_tp
    part = share // 2

    def fits(index):
        owner = (tp_at - index // part + n_tp) % n_tp
        return token == owner * share + ((lane // each) % 2) * part + index % part

    first = jnp.where(fits(place_at), 1.0, 0.0)
    second = jnp.where((place_at < 2 * CAP) & fits(place_at + each), 1.0, 0.0)
    for i, table in enumerate((first, second + high, weight - high)):
        place_ref[i] = table.astype(BF16)


def tables_kernel(ids_hbm, weights_hbm, after, taken_ref, place_ref, ids, weights, sems):
    copies = [
        pltpu.make_async_copy(ids_hbm, ids, sems.at[0]),
        pltpu.make_async_copy(weights_hbm, weights, sems.at[1]),
    ]
    for copy in copies:
        copy.start()
    for copy in copies:
        copy.wait()
    route_tables(ids, weights, taken_ref, place_ref)


def tables(n_tp, chips, seqs, ids, weights, after):
    return pl.pallas_call(
        tables_kernel,
        name="tables",
        out_shape=(
            pltpu.VMEM((2, chips * 2 * n_tp, n_tp * seqs), BF16),
            pltpu.VMEM((3, seqs, chips * 2 * n_tp), BF16),
        ),
        in_specs=[ANY] * 3,
        out_specs=(IN_VMEM,) * 2,
        scratch_shapes=[
            pltpu.VMEM(ids.shape, ids.dtype),
            pltpu.VMEM(weights.shape, weights.dtype),
            pltpu.SemaphoreType.DMA((2,)),
        ],
        compiler_params=pltpu.CompilerParams(vmem_limit_bytes=8 * MIB),
    )(at_hbm(ids), at_hbm(weights), after)


def pack_kernel(*refs):
    dense, packed, sems = refs[:3], refs[3], refs[4]
    copies, at = [], 0
    for i, source in enumerate(dense):
        into = packed.at[:, at : at + source.shape[1]]
        copies.append(pltpu.make_async_copy(source, into, sems.at[i]))
        at += source.shape[1]
    for copy in copies:
        copy.start()
    for copy in copies:
        copy.wait()


def pack(dense):
    return pl.pallas_call(
        pack_kernel,
        name="pack",
        out_shape=pltpu.VMEM((dense[0].shape[0], sum(w.shape[1] for w in dense)), BF16),
        in_specs=[ANY] * 3,
        out_specs=IN_VMEM,
        scratch_shapes=[pltpu.SemaphoreType.DMA((3,))],
        compiler_params=pltpu.CompilerParams(vmem_limit_bytes=1 * MIB),
    )(*[at_hbm(w) for w in dense])


def attend_kernel(chunks, forget_bias, lens_hbm, after, *refs):
    ahead, refs = refs[:3], refs[3:]
    sources, out_ref, fetched, rest = refs[:11], refs[11], refs[12:15], refs[15:]
    held, (lens, queries, keys, values, shift, scores, mixed, sems) = rest[:11], rest[11:]
    tok, gain, wq, wk, wv, wf, qg, kg, cum, wo, cache = held
    seqs, slots, pair = cache.shape
    head = qg.shape[1]
    group = wq.shape[1] // head
    copies = [pltpu.make_async_copy(sources[i], held[i], sems.at[i]) for i in range(10)]
    step = seqs // chunks
    parts = [
        pltpu.make_async_copy(
            sources[10].at[pl.ds(i * step, step)], cache.at[pl.ds(i * step, step)], sems.at[10 + i]
        )
        for i in range(chunks)
    ]
    lens_copy = pltpu.make_async_copy(lens_hbm, lens, sems.at[10 + chunks])
    fetches = [pltpu.make_async_copy(ahead[i], fetched[i], sems.at[11 + chunks + i]) for i in range(3)]
    lens_copy.start()
    for copy in copies[:9]:
        copy.start()
    for part in parts:
        part.start()
    copies[9].start()
    for copy in copies[:8]:
        copy.wait()

    normed = normal_rows(tok[...].astype(F32), gain[...]).astype(BF16)
    query_raw = dot(normed, wq[...])
    key_new = normal_rows(dot_nt(normed, wk[...]), kg[...]).astype(BF16).astype(F32)
    value_new = dot_nt(normed, wv[...]).astype(BF16).astype(F32)
    blank = jnp.zeros((seqs, pair - head), F32)
    key_new = jnp.concatenate([key_new, blank], axis=1)
    value_new = jnp.concatenate([blank, value_new], axis=1)
    for h in range(group):
        query = normal_rows(query_raw[:, h * head : (h + 1) * head], qg[...])
        query = jnp.concatenate([query.astype(BF16).astype(F32), blank], axis=1)
        queries[pl.ds(h, seqs, stride=group), :] = query
        keys[pl.ds(h, seqs, stride=group), :] = key_new
        values[pl.ds(h, seqs, stride=group), :] = value_new
    forget = jnp.sum(normed.astype(F32) * wf[...].astype(F32), axis=1, keepdims=True) + forget_bias[0]
    log_gate = jnp.minimum(forget, 0.0) - jnp.log1p(jnp.exp(-jnp.abs(forget)))

    lens_copy.wait()
    row = rows_of((seqs, 1))
    length = jnp.zeros((seqs, 1), jnp.int32)
    for s in range(seqs):
        length = jnp.where(row == s, lens[s], length)
    copies[8].wait()
    position = lanes_of((seqs, slots))
    summed = cum[...].reshape(seqs, slots)
    last = jnp.sum(jnp.where(position == length - 1, summed, 0.0), axis=1, keepdims=True)
    shift[...] = jnp.where(position < length, (last + log_gate) - summed, -jnp.inf)

    multiplier = head ** (-0.5)
    own_score = jnp.sum(queries[...] * keys[...], axis=1, keepdims=True) * multiplier
    tall = 2 * group
    upper = rows_of((tall, 1)) < group
    for p in range(seqs // 2):
        if (2 * p) % step == 0:
            parts[2 * p // step].wait()
            if 2 * p // step == 0:
                for fetch in fetches:
                    fetch.start()
        query = queries[tall * p : tall * (p + 1), :].astype(BF16)
        score = jnp.where(upper, dot_nt(query, cache[2 * p]), dot_nt(query, cache[2 * p + 1]))
        moved = jnp.where(upper, shift[2 * p : 2 * p + 1, :], shift[2 * p + 1 : 2 * p + 2, :])
        scores[tall * p : tall * (p + 1), :] = score * multiplier + moved
    score = scores[...]
    peak = jnp.maximum(jnp.max(score, axis=1, keepdims=True), own_score)
    past = jnp.exp(score - peak)
    own = jnp.exp(own_score - peak)
    whole = 1.0 / (jnp.sum(past, axis=1, keepdims=True) + own)
    scores[...] = past * whole
    own_prob = (own * whole).astype(BF16).astype(F32)
    for p in range(seqs // 2):
        prob = scores[tall * p : tall * (p + 1), :].astype(BF16)
        mixed[tall * p : tall * (p + 1), :] = jnp.where(
            upper, dot(prob, cache[2 * p]), dot(prob, cache[2 * p + 1])
        )
    mixed[...] = mixed[...] + own_prob * values[...]
    copies[9].wait()
    total = jnp.zeros((seqs, wo.shape[1]), F32)
    for h in range(group):
        mix = mixed[pl.ds(h, seqs, stride=group), :][:, pair - head :].astype(BF16)
        total = total + dot(mix, wo[h * head : (h + 1) * head, :])
    partial = total.astype(BF16)
    out_ref[...] = partial
    for fetch in fetches:
        fetch.wait()


def attend(lens, forget_bias, after, ahead, *arrays):
    chunks = 4
    tok, wq, qg, cache = arrays[0], arrays[2], arrays[6], arrays[10]
    seqs, slots, pair = cache.shape
    heads = wq.shape[1] // qg.shape[1]
    rows = seqs * heads
    scratch = [pltpu.VMEM(a.shape, a.dtype) for a in arrays]
    scratch += [pltpu.SMEM(lens.shape, lens.dtype)]
    scratch += [pltpu.VMEM((rows, pair), F32)] * 3
    scratch += [pltpu.VMEM((seqs, slots), F32), pltpu.VMEM((rows, slots), F32), pltpu.VMEM((rows, pair), F32)]
    scratch += [pltpu.SemaphoreType.DMA((14 + chunks,))]
    return pl.pallas_call(
        functools.partial(attend_kernel, chunks),
        name="attend",
        out_shape=(pltpu.VMEM(tok.shape, BF16), *(pltpu.VMEM(w.shape, BF16) for w in ahead)),
        in_specs=[IN_SMEM] + [ANY] * 16,
        out_specs=(IN_VMEM,) * 4,
        scratch_shapes=scratch,
        compiler_params=pltpu.CompilerParams(vmem_limit_bytes=16 * MIB),
    )(forget_bias, at_hbm(lens), after, *[at_hbm(a) for a in (*ahead, *arrays)])


def send_kernel(n_tp, *refs):
    crossed, (tok, gain, taken_ref), (message, own_residual) = refs[:n_tp], refs[n_tp : n_tp + 3], refs[-2:]
    seqs, width = tok.shape
    rows = message.shape[0]
    span = width // n_tp
    share = seqs // n_tp
    tp_at = lax.axis_index("tp")
    attn_out = crossed[0][...].astype(F32)
    for t in range(1, n_tp):
        attn_out = attn_out + crossed[t][...].astype(F32)
    residual = (tok[...].astype(F32) + attn_out).astype(BF16)
    residual_f = residual.astype(F32)
    kept = residual[:, :span]
    for t in range(1, n_tp):
        kept = jnp.where(tp_at == t, residual[:, t * span : (t + 1) * span], kept)
    own_residual[...] = kept
    normed = normal_rows(residual_f, gain[...])
    pieces = jnp.concatenate([normed[:, q * span : (q + 1) * span] for q in range(n_tp)], axis=0)
    pieces = pieces.astype(BF16)
    wide = n_tp * seqs
    for o in range(2):
        message[:, o * span : (o + 1) * span] = dot(taken_ref[o], pieces).astype(BF16)
    each = 2 * n_tp
    both = 2 * each
    part = share // 2
    narrow = span // 2
    row, lane = rows_of((both, wide)), lanes_of((both, wide))
    token = tp_at * share + (row // each) * part + (row % each) // n_tp
    fits = (lane // seqs == row % n_tp) & (lane % seqs == token)
    block = dot(jnp.where(fits, 1.0, 0.0).astype(BF16), pieces).astype(BF16)
    block = jnp.broadcast_to(block[None], (rows // both, both, span)).reshape(rows, span)
    message[:, 2 * span : 3 * span] = block
    pieces = jnp.concatenate([normed[:, q * narrow : (q + 1) * narrow] for q in range(each)], axis=0)
    row, lane = rows_of((both, each * seqs)), lanes_of((both, each * seqs))
    token = tp_at * share + (row // each) * part + part - 1
    fits = (lane // seqs == row % each) & (lane % seqs == token)
    block = dot(jnp.where(fits, 1.0, 0.0).astype(BF16), pieces.astype(BF16)).astype(BF16)
    block = jnp.broadcast_to(block[None], (rows // both, both, narrow)).reshape(rows, narrow)
    message[:, 3 * span :] = block


def send(crossed, tok, gain, taken, chips, swapped):
    n_tp = len(crossed)
    seqs, width = tok.shape
    span = width // n_tp
    rows = chips * 2 * n_tp
    return pl.pallas_call(
        functools.partial(send_kernel, n_tp),
        name="send",
        out_shape=(
            pltpu.VMEM((rows, 3 * span + span // 2), BF16),
            pltpu.VMEM((seqs, span), BF16),
        ),
        in_specs=[IN_VMEM] * (n_tp + 3) + [ANY] * len(swapped),
        out_specs=(IN_VMEM, IN_VMEM),
        compiler_params=pltpu.CompilerParams(vmem_limit_bytes=8 * MIB),
    )(*[at_vmem(part) for part in crossed], tok, gain, at_vmem(taken), *swapped)


def experts_kernel(n_tp, arrived, shared, *refs):
    own, swapped, shards_of, refs = refs[:3], refs[3:6], refs[6:10], refs[10:]
    blocks, (down, spread) = refs[:n_tp], refs[n_tp:]
    tp_at = lax.axis_index("tp")
    width = shared.shape[0] * shared.shape[1]
    rows, span = arrived.shape[0], blocks[0].shape[1]
    each = 2 * n_tp
    chips = rows // each
    for j in range(spread.shape[0]):
        spread[j] = arrived[:, j * LANES : (j + 1) * LANES].astype(F32)

    def gathered(k, column):
        return jnp.concatenate(
            [
                spread[column // LANES + j, pl.ds(k * n_tp + q, chips, stride=each), :]
                for q in range(n_tp)
                for j in range(span // LANES)
            ],
            axis=1,
        )

    last = [spread[3 * span // LANES, pl.ds(i, chips, stride=each), :] for i in range(each)]
    tokens = [gathered(0, 2 * span), gathered(1, 2 * span), jnp.concatenate(last, axis=1)]
    tokens = jnp.concatenate(tokens, axis=0).astype(BF16)
    gate_row = shared[...].astype(F32)
    gate_row = jnp.concatenate([gate_row[i : i + 1] for i in range(gate_row.shape[0])], axis=1)
    gate_rows = jnp.broadcast_to(gate_row, (8, gate_row.shape[1])).astype(BF16)
    mix_gate = dot_nt(tokens, gate_rows)[:, :1]
    mix_gate = 1.0 / (1.0 + jnp.exp(-mix_gate))
    gate = dot_nt(tokens, jnp.concatenate([w[:, :width] for w in shards_of], axis=0))
    up = dot_nt(tokens, jnp.concatenate([w[:, width : 2 * width] for w in shards_of], axis=0))
    down[...] = jnp.concatenate([w[:, 2 * width :] for w in shards_of], axis=0)
    hidden = (mix_gate * (gate / (1.0 + jnp.exp(-gate)) * up)).astype(BF16)
    taken = chips * 2 * CAP
    for block in blocks:
        block[taken:, :] = hidden
    for o in range(2):
        tokens = [gathered(k, o * span) for k in range(CAP)]
        tokens = jnp.concatenate(tokens, axis=0).astype(BF16)
        gate_w, up_w, down_w = (own, swapped)[o]
        gate = dot(tokens, gate_w[...])
        up = dot(tokens, up_w[...])
        hidden = (gate / (1.0 + jnp.exp(-gate)) * up).astype(BF16)
        part = dot(hidden, down_w[...]).astype(BF16)
        parts = [part[:, t * span : (t + 1) * span] for t in range(n_tp)]
        for k in range(n_tp):
            chosen = parts[k]
            for t in range(1, n_tp):
                chosen = jnp.where(tp_at == t, parts[(t + k) % n_tp], chosen)
            blocks[k][o * chips * CAP : (o + 1) * chips * CAP, :] = chosen


def experts(n_tp, span, arrived, shared, own, swapped, shards_of):
    rows = arrived.shape[0]
    chips = rows // (2 * n_tp)
    units = sum(w.shape[0] for w in shards_of)
    return pl.pallas_call(
        functools.partial(experts_kernel, n_tp),
        name="experts",
        out_shape=(
            *[pltpu.VMEM((chips * 2 * CAP + chips * 3, span), BF16)] * n_tp,
            pltpu.VMEM((units, span), BF16),
        ),
        in_specs=[IN_VMEM] * 12,
        out_specs=(IN_VMEM,) * (n_tp + 1),
        scratch_shapes=[pltpu.VMEM((arrived.shape[1] // LANES, rows, LANES), F32)],
        compiler_params=pltpu.CompilerParams(vmem_limit_bytes=8 * MIB),
    )(at_vmem(arrived), shared, *[at_vmem(w) for w in (*own, *swapped, *shards_of)])


def combine_kernel(n_tp, *refs):
    crossed, (down, out_ref, spread) = refs[:n_tp], refs[n_tp:]
    span = down.shape[1]
    chips, each, _ = out_ref.shape
    block = chips * CAP
    taken = 2 * block
    total = crossed[0][:taken].astype(F32)
    for t in range(1, n_tp):
        total = total + crossed[t][:taken].astype(F32)
    parts = []
    for t in range(n_tp):
        part = dot(crossed[t][taken:], down[...])
        parts += [part[k * chips : (k + 1) * chips] for k in range(part.shape[0] // chips)]
    parts += [total[i * chips : (i + 1) * chips] for i in range(2 * CAP)]
    for i, part in enumerate(parts):
        for j in range(span // LANES):
            spread[i // each * (span // LANES) + j, pl.ds(i % each, chips, stride=each), :] = part[
                :, j * LANES : (j + 1) * LANES
            ]
    for j in range(spread.shape[0]):
        column = spread[j].astype(BF16).reshape(chips, each, LANES)
        out_ref[:, :, j * LANES : (j + 1) * LANES] = column


def combine(crossed, down, chips):
    n_tp, span = len(crossed), down.shape[1]
    each = 2 * n_tp
    return pl.pallas_call(
        functools.partial(combine_kernel, n_tp),
        name="combine",
        out_shape=pltpu.VMEM((chips, each, 2 * span), BF16),
        in_specs=[IN_VMEM] * (n_tp + 1),
        out_specs=IN_VMEM,
        scratch_shapes=[pltpu.VMEM((2 * span // LANES, chips * each, LANES), F32)],
        compiler_params=pltpu.CompilerParams(vmem_limit_bytes=8 * MIB),
    )(*[at_vmem(block) for block in crossed], at_vmem(down))


def finish_kernel(arrived, place, residual, out_ref):
    span = residual.shape[1]
    left, right = arrived[:, :span], arrived[:, span:]
    total = dot(place[0], left) + (dot(place[1], right) + dot(place[2], right))
    out_ref[...] = (residual[...].astype(F32) + total).astype(BF16)


def finish(arrived, place, residual):
    return pl.pallas_call(
        finish_kernel,
        name="finish",
        out_shape=jax.ShapeDtypeStruct(residual.shape, BF16),
        in_specs=[IN_VMEM] * 3,
        out_specs=IN_VMEM,
        compiler_params=pltpu.CompilerParams(vmem_limit_bytes=8 * MIB),
    )(at_vmem(arrived), at_vmem(place), at_vmem(residual))


def shards(
    tokens,
    attn_gain,
    w_query,
    w_key,
    w_value,
    w_forget,
    forget_bias,
    query_gain,
    key_gain,
    cache_pairs,
    cache_cum,
    lengths,
    w_output,
    ffn_gain,
    expert_ids,
    route_weight,
    w_exp_gate,
    w_exp_up,
    w_exp_down,
    shared_gate,
    w_dense_gate,
    w_dense_up,
    w_dense_down,
):
    seqs, width = tokens.shape
    n_tp, chips = lax.axis_size("tp"), lax.axis_size(FAR)
    span = width // n_tp

    def other(w):
        return lax.ppermute(w, "ep_2", [(0, 1), (1, 0)])

    def neighbour(w, flip):
        axes = ("ep_1", "ep_2")
        return lax.ppermute(w, axes, [(i, i ^ flip) for i in range(lax.axis_size(axes))])

    def passed_on(x, k):
        return lax.ppermute(x, "tp", [(i, (i + k) % n_tp) for i in range(n_tp)])

    own = [w_exp_gate[0], w_exp_up[0], w_exp_down[0]]
    swapped = [other(w) for w in own]
    packed = pack((w_dense_gate, w_dense_up, w_dense_down))
    near, far, across = neighbour(packed, 2), neighbour(packed, 3), neighbour(packed, 1)
    partial, *fetched = attend(
        lengths,
        forget_bias,
        packed,
        own,
        tokens,
        attn_gain[None],
        w_query,
        w_key.T,
        w_value.T,
        w_forget.T,
        query_gain[None],
        key_gain[None],
        cache_cum,
        w_output,
        cache_pairs[:, 0],
    )
    crossed = [partial] + [passed_on(partial, k) for k in HEADS_ORDER]
    taken, place = tables(n_tp, chips, seqs, expert_ids.T, route_weight.T, partial)
    message, own_residual = send(crossed, tokens, ffn_gain[None], taken, chips, [*swapped, near, across, far])
    arrived = lax.all_to_all(message.reshape(chips, -1, message.shape[1]), FAR, 0, 0, tiled=True)
    *blocks, down = experts(
        n_tp,
        span,
        arrived.reshape(message.shape),
        shared_gate.reshape(-1, LANES),
        fetched,
        swapped,
        (packed, near, across, far),
    )
    crossed = [passed_on(blocks[k], k) for k in EXPERT_ORDER]
    crossed = [blocks[0]] + [crossed[EXPERT_ORDER.index(k)] for k in range(1, n_tp)]
    total = combine(crossed, down, chips)
    arrived = lax.all_to_all(total, FAR, 0, 0, tiled=True)
    return finish(arrived.reshape(-1, arrived.shape[2]), place, own_residual)


def solution(mesh):
    split = Mesh(mesh.devices.reshape(8, 4, 2, mesh.shape["tp"]), ("ep_0", "ep_1", "ep_2", "tp"))
    return jax.shard_map(
        shards,
        mesh=split,
        in_specs=(
            P(EP, None),
            P(),
            P(None, "tp"),
            P(None, "tp"),
            P(None, "tp"),
            P(None, "tp"),
            P("tp"),
            P(),
            P(),
            P(EP, "tp", None, None),
            P(EP, "tp", None),
            P(EP),
            P("tp", None),
            P(),
            P(),
            P(),
            P(EP, None, "tp"),
            P(EP, None, "tp"),
            P(EP, "tp", None),
            P(),
            P(EP, None),
            P(EP, None),
            P(EP, "tp"),
        ),
        out_specs=P(EP, "tp"),
        check_vma=False,
    )
```
